256 devices in a mesh: ep: 64 (over z, y, core), tp: 4 (over x).
Axes of the slice: x: 4, y: 4, z: 8, core: 2. Of those that a mesh axis runs over, the one named last changes fastest.
Arguments:
- tokens: bfloat16 [1024, 2048], P('ep', 'tp'), may hold values from -40 to 40
- kv_cache: bfloat16 [1024, 1024, 512], P('ep', None, 'tp'), may hold values from -1000 to 1000
- cum_gate: float32 [1024, 16, 1024], P('ep', 'tp'), may hold values from -400 to 0, as said below
- lengths: int32 [1024], P('ep'), may hold values from 256 to 1024
- w_query: bfloat16 [2048, 1024], P(None, 'tp'), may hold values from -0.125 to 0.125
- w_key: bfloat16 [2048, 256], P(None, 'tp'), may hold values from -0.125 to 0.125
- w_value: bfloat16 [2048, 256], P(None, 'tp'), may hold values from -0.125 to 0.125
- w_forget: bfloat16 [2048, 16], P(None, 'tp'), may hold values from -0.5 to 0.5
- forget_bias: float32 [16], P('tp'), may hold values from -2.5 to 1.5
- w_out: bfloat16 [1024, 2048], P('tp'), may hold values from -0.1875 to 0.1875
- attn_gain: bfloat16 [2048], replicated, may hold values from 0.099609375 to 1.8984375
- ffn_gain: bfloat16 [2048], replicated, may hold values from 0.099609375 to 1.8984375
- mix_gate: bfloat16 [2048], replicated, may hold values from -0.125 to 0.125
- expert_gate: bfloat16 [64, 2048, 1024], P('ep', None, 'tp'), may hold values from -0.125 to 0.125
- expert_up: bfloat16 [64, 2048, 1024], P('ep', None, 'tp'), may hold values from -0.125 to 0.125
- expert_down: bfloat16 [64, 1024, 2048], P('ep', 'tp'), may hold values from -0.1875 to 0.1875
- chosen: int32 [1024, 2], P('ep'), may hold values from 0 to 63, as said below
- route_weight: float32 [1024, 2], P('ep'), may hold values from 0.5 to 1.5
- dense_gate: bfloat16 [2048, 1024], P(None, 'tp'), may hold values from -0.125 to 0.125
- dense_up: bfloat16 [2048, 1024], P(None, 'tp'), may hold values from -0.125 to 0.125
- dense_down: bfloat16 [1024, 2048], P('tp'), may hold values from -0.1875 to 0.1875
Outputs:
- mixed: bfloat16 [1024, 2048], P('ep', 'tp')
The draws below stay inside these ranges and needn't reach their ends.
Inputs may be any that keep to these rules, and one draw needn't show every extreme that they name: `cum_gate`: along positions each row never rises: entry p is the sum of the log forget gates of positions 0 to p of that sequence and head. `chosen`: each row names two different experts of one group of 8 consecutive expert numbers. The rows of one device name any one expert at most 2 times, and some expert exactly 2 times.
All inputs are finite; a program needn't handle non-finite values.
Results may differ from the reference program's by a relative error of at most 0.014.
Values may be sent and summed in bfloat16 or wider, within the bound.
A program may use at most 64 MiB of HBM per device.

```python
import jax
import jax.numpy as jnp
from jax import lax

D = 2048
QUERY_HEADS = 16
KVH = 4
HD = 64
DE = 1024
DF = 1024
EPG = 8
TOP = 2
CACHED_POSITIONS = 1024
SEQ_DEV = 16
SEQUENCE_TOTAL = 1024
EXPERTS = 64
CAP = 2
N_EP = 64
N_TP = 4


def draw_tokens(key, part):
    first, second, third = jax.random.split(key, 3)
    column_pos = jnp.arange(D, dtype=jnp.float32) / D
    entries = jax.random.normal(first, (SEQUENCE_TOTAL, D), jnp.float32)
    column_scale = 3.0 ** column_pos
    row_scale = jnp.exp(jax.random.uniform(second, (SEQUENCE_TOTAL, 1), jnp.float32, jnp.log(0.5), jnp.log(2.0)))
    roughness = jnp.exp(jax.random.uniform(third, (1, D), jnp.float32, jnp.log(0.5), jnp.log(2.0)))
    return (entries * 0.6 * column_scale[None, :] * roughness * row_scale).astype(jnp.bfloat16)


def draw_kv_cache(key, part):
    first = jax.random.fold_in(key, 0)
    total_width = 2 * KVH * HD
    entries = jax.random.normal(first, (SEQUENCE_TOTAL, CACHED_POSITIONS, total_width), jnp.float32)
    return entries.astype(jnp.bfloat16)


def draw_cum_gate(key, part):
    key_rows = jax.random.split(key, 7)
    scores_int = jax.random.randint(key_rows[0], (SEQUENCE_TOTAL, QUERY_HEADS), 0, 2 ** 20) * QUERY_HEADS + jnp.arange(QUERY_HEADS, dtype=jnp.int32)[None, :]
    ranking = jnp.argsort(jnp.argsort(scores_int, axis=1), axis=1)
    slow_count = QUERY_HEADS // 2
    slow = (ranking < slow_count)[:, :, None]
    slow_rate = jnp.exp(jax.random.uniform(key_rows[1], (SEQUENCE_TOTAL, QUERY_HEADS, 1), jnp.float32, jnp.log(0.2), jnp.log(0.8))) / CACHED_POSITIONS
    fast_rate = jnp.exp(jax.random.uniform(key_rows[2], (SEQUENCE_TOTAL, QUERY_HEADS, 1), jnp.float32, jnp.log(0.01), jnp.log(1.0 / 30.0)))
    rate_all = jnp.where(slow, slow_rate, fast_rate)
    block_factor = jnp.exp(jax.random.uniform(key_rows[3], (SEQUENCE_TOTAL, 1, CACHED_POSITIONS // 128), jnp.float32, jnp.log(0.5), jnp.log(2.0)))
    block_factor = jnp.repeat(block_factor, 128, axis=2)
    roughness = jnp.exp(jax.random.uniform(key_rows[4], (SEQUENCE_TOTAL, QUERY_HEADS, CACHED_POSITIONS), jnp.float32, jnp.log(0.5), jnp.log(2.0)))
    stepping_through = -rate_all * block_factor * roughness
    group_position = jax.random.randint(key_rows[5], (SEQUENCE_TOTAL, QUERY_HEADS, 2), 0, CACHED_POSITIONS)
    group_length = jnp.log(jax.random.uniform(key_rows[6], (SEQUENCE_TOTAL, QUERY_HEADS, 2), jnp.float32, 0.5, 0.8))
    position_rows = jnp.arange(CACHED_POSITIONS, dtype=jnp.int32)
    position_groups = jnp.sum(jnp.where(position_rows[None, None, None, :] == group_position[:, :, :, None], group_length[:, :, :, None], 0.0), axis=2)
    return jnp.cumsum(stepping_through + position_groups, axis=-1).astype(jnp.float32)


def draw_chosen(key, part):
    pair_count = EXPERTS // 2

    def one_block(block_key):
        key_perm, key_first, key_rest, key_order = jax.random.split(block_key, 4)
        group_keys = jax.random.split(key_perm, EXPERTS // EPG)

        def shuffle_group(group_key):
            return jax.random.permutation(group_key, EPG).astype(jnp.int32)
        shuffled = jax.vmap(shuffle_group)(group_keys)
        offsets = (jnp.arange(EXPERTS // EPG, dtype=jnp.int32) * EPG)[:, None]
        members = (shuffled + offsets).reshape(pair_count, 2).astype(jnp.int32)
        first_pair = jax.random.randint(key_first, (), 0, pair_count).astype(jnp.int32)
        others = (jax.random.permutation(key_rest, (pair_count - 1) * CAP)[:SEQ_DEV - CAP] // CAP).astype(jnp.int32)
        others = others + (others >= first_pair).astype(jnp.int32)
        pairs = jnp.concatenate([jnp.full((CAP,), first_pair, jnp.int32), others])
        pairs = pairs[jax.random.permutation(key_order, SEQ_DEV)]
        return members[pairs]
    block_keys = jax.random.split(key, N_EP)
    return jax.vmap(one_block)(block_keys).reshape(SEQ_DEV * N_EP, TOP).astype(jnp.int32)


def with_ends(result, rng, smallest, high):
    longest = result.shape.index(max(result.shape))
    spots = []
    for shift in (0, 1):
        where = [jax.random.randint(jax.random.fold_in(rng, axis), (), 0, length) for axis, length in enumerate(result.shape)]
        where[longest] = (where[longest] + shift) % result.shape[longest]
        spots.append(tuple(where))
    return result.at[spots[0]].set(smallest).at[spots[1]].set(high)


def level_of(own_key, extent, pieces, smallest, high):
    level, own = 1.0, jax.random.fold_in(own_key, 6)
    for axis_at, shards_of in pieces:
        draws = jnp.exp(jax.random.uniform(jax.random.fold_in(own, axis_at), (shards_of,), jnp.float32, smallest / len(pieces), high / len(pieces)))
        level = level * jnp.repeat(draws, extent[axis_at] // shards_of).reshape([-1 if axis == axis_at else 1 for axis in range(len(extent))])
    return level


def normal_values(own_key, extent, width, reach, cuts=(), kind=jnp.bfloat16):
    array = jax.random.normal(own_key, extent, jnp.float32) * width
    if len(cuts) > 0:
        array = level_of(own_key, extent, cuts, -0.22, 0.18) * array
    return jnp.clip(array, min=-reach, max=reach).astype(kind)


def setup_inputs(seed: int = 0) -> dict:
    key_of = jax.random.split(jax.random.key(seed), 22)
    tokens = draw_tokens(jax.random.fold_in(key_of[21], 71), 0)
    kv_cache = draw_kv_cache(jax.random.fold_in(key_of[21], 71), 0)
    cum_gate = draw_cum_gate(jax.random.fold_in(key_of[21], 71), 0)
    lengths = with_ends(jax.random.randint(key_of[3], (SEQUENCE_TOTAL,), CACHED_POSITIONS // 4, CACHED_POSITIONS + 1), jax.random.fold_in(key_of[3], 1), CACHED_POSITIONS // 4, CACHED_POSITIONS).astype(jnp.int32)
    w_query = normal_values(key_of[4], (D, QUERY_HEADS * HD), D ** -0.5, 0.125, ((1, 4),))
    w_key = normal_values(key_of[5], (D, KVH * HD), D ** -0.5, 0.125, ((1, 4),))
    w_value = normal_values(key_of[6], (D, KVH * HD), D ** -0.5, 0.125, ((1, 4),))
    w_forget = normal_values(key_of[7], (D, QUERY_HEADS), (D // 16) ** -0.5, 0.5, ((1, 4),))
    forget_bias = jnp.clip(-2.5 + 4.0 * jax.random.uniform(key_of[8], (QUERY_HEADS,), jnp.float32) ** level_of(key_of[8], (QUERY_HEADS,), ((0, 4),), -0.2, 0.2), -2.5, 1.5)
    w_out = normal_values(key_of[9], (QUERY_HEADS * HD, D), (QUERY_HEADS * HD) ** -0.5, 0.1875, ((0, 4),))
    attn_gain = jnp.clip(1.0 + 0.18 * jax.random.normal(key_of[10], (D,), jnp.float32), 0.099609375, 1.8984375).astype(jnp.bfloat16)
    ffn_gain = jnp.clip(1.0 + 0.18 * jax.random.normal(key_of[11], (D,), jnp.float32), 0.099609375, 1.8984375).astype(jnp.bfloat16)
    mix_gate = normal_values(key_of[12], (D,), D ** -0.5, 0.125)
    expert_gate = normal_values(key_of[13], (EXPERTS, D, DE), D ** -0.5, 0.125, ((0, 64), (2, 4)))
    expert_up = normal_values(key_of[14], (EXPERTS, D, DE), D ** -0.5, 0.125, ((0, 64), (2, 4)))
    expert_down = normal_values(key_of[15], (EXPERTS, DE, D), DE ** -0.5, 0.1875, ((0, 64), (1, 4)))
    chosen = draw_chosen(jax.random.fold_in(key_of[21], 71), 0)
    route_weight = jnp.clip(0.5 + 1.0 * jax.random.uniform(key_of[17], (SEQUENCE_TOTAL, TOP), jnp.float32) ** level_of(key_of[17], (SEQUENCE_TOTAL, TOP), ((0, 64),), -0.2, 0.2), 0.5, 1.5)
    dense_gate = normal_values(key_of[18], (D, DF), D ** -0.5, 0.125, ((1, 4),))
    dense_up = normal_values(key_of[19], (D, DF), D ** -0.5, 0.125, ((1, 4),))
    dense_down = normal_values(key_of[20], (DF, D), DF ** -0.5, 0.1875, ((0, 4),))
    return {"tokens": tokens, "kv_cache": kv_cache, "cum_gate": cum_gate, "lengths": lengths, "w_query": w_query, "w_key": w_key, "w_value": w_value, "w_forget": w_forget, "forget_bias": forget_bias, "w_out": w_out, "attn_gain": attn_gain, "ffn_gain": ffn_gain, "mix_gate": mix_gate, "expert_gate": expert_gate, "expert_up": expert_up, "expert_down": expert_down, "chosen": chosen, "route_weight": route_weight, "dense_gate": dense_gate, "dense_up": dense_up, "dense_down": dense_down}


epsilon = 1e-06

def norm_rows(values, scales):
    widened = values.astype(jnp.float32)
    square = lax.optimization_barrier(jnp.mean(widened * widened, axis=-1, keepdims=True))
    return (widened * lax.rsqrt(square + epsilon) * scales.astype(jnp.float32)).astype(jnp.bfloat16)

def split_sum(left, right):
    piece_width = left.shape[1] // N_TP
    running = jnp.zeros((left.shape[0], right.shape[1]), jnp.float32)
    for member in range(N_TP):
        lower = member * piece_width
        partial_value = jnp.dot(left[:, lower:lower + piece_width], right[lower:lower + piece_width], preferred_element_type=jnp.float32).astype(jnp.bfloat16)
        partial_value = lax.optimization_barrier(partial_value)
        running = running + partial_value.astype(jnp.float32)
    return running

def reference(tokens, kv_cache, cum_gate, lengths, w_query, w_key, w_value, w_forget, forget_bias, w_out, attn_gain, ffn_gain, mix_gate, expert_gate, expert_up, expert_down, chosen, route_weight, dense_gate, dense_up, dense_down):
    group_size = QUERY_HEADS // KVH
    score_scale = HD ** (-0.5)
    h_one = norm_rows(tokens, attn_gain)
    queries = jnp.dot(h_one, w_query, preferred_element_type=jnp.float32).astype(jnp.bfloat16)
    key_new = jnp.dot(h_one, w_key, preferred_element_type=jnp.float32).astype(jnp.bfloat16)
    value_new = jnp.dot(h_one, w_value, preferred_element_type=jnp.float32).astype(jnp.bfloat16)
    log_forget = jax.nn.log_sigmoid(jnp.dot(h_one, w_forget, preferred_element_type=jnp.float32) + forget_bias)

    def one_sequence(packed):
        query_row, key_row, value_row, forget_row, cache_row, gate_row, length_one = packed
        query_heads = query_row.astype(jnp.float32).reshape(KVH, group_size, HD)
        stacked = cache_row.astype(jnp.float32).reshape(CACHED_POSITIONS, KVH, 2, HD)
        scores = jnp.einsum('jgd,cjd->jgc', query_heads, stacked[:, :, 0, :]) * score_scale
        gate_rows = gate_row.reshape(KVH, group_size, CACHED_POSITIONS)
        latest = lax.dynamic_index_in_dim(gate_rows, (length_one - 1).astype(jnp.int32), axis=2, keepdims=True)
        scores = scores + latest - gate_rows + forget_row.reshape(KVH, group_size)[:, :, None]
        position_rows = jnp.arange(CACHED_POSITIONS, dtype=jnp.int32)
        scores = jnp.where(position_rows[None, None, :] < length_one, scores, -jnp.inf)
        own_score = jnp.einsum('jgd,jd->jg', query_heads, key_row.astype(jnp.float32).reshape(KVH, HD)) * score_scale
        highest = jnp.maximum(lax.optimization_barrier(jnp.max(scores, axis=-1)), own_score)
        weights = jnp.exp(scores - highest[:, :, None])
        own_weight = jnp.exp(own_score - highest)
        denominator = lax.optimization_barrier(jnp.sum(weights, axis=-1)) + own_weight
        weights = (weights / denominator[:, :, None]).astype(jnp.bfloat16)
        own_weight = (own_weight / denominator).astype(jnp.bfloat16)
        blended = jnp.einsum('jgc,cjd->jgd', weights.astype(jnp.float32), stacked[:, :, 1, :])
        blended = blended + own_weight.astype(jnp.float32)[:, :, None] * value_row.astype(jnp.float32).reshape(KVH, 1, HD)
        return blended.astype(jnp.bfloat16).reshape(QUERY_HEADS * HD)
    head_out = lax.map(one_sequence, (queries, key_new, value_new, log_forget, kv_cache, cum_gate, lengths))
    attention = split_sum(head_out, w_out)
    residual = (tokens.astype(jnp.float32) + attention).astype(jnp.bfloat16)
    h_two = norm_rows(residual, ffn_gain)
    flat_routes = chosen.reshape(N_EP, SEQ_DEV * TOP)
    one_hot = (flat_routes[:, :, None] == jnp.arange(EXPERTS, dtype=jnp.int32)[None, None, :]).astype(jnp.int32)
    earlier = (jnp.cumsum(one_hot, axis=1) - one_hot).astype(jnp.int32)
    rank_of = lax.optimization_barrier(jnp.sum(earlier * one_hot, axis=-1)).astype(jnp.int32)
    slot_of = (jnp.arange(N_EP, dtype=jnp.int32)[:, None] * CAP + rank_of).reshape(-1).astype(jnp.int32)
    expert_of = flat_routes.reshape(-1).astype(jnp.int32)
    source_rows = (jnp.arange(SEQUENCE_TOTAL * TOP, dtype=jnp.int32) // TOP).astype(jnp.int32)
    buffer = jnp.zeros((EXPERTS, N_EP * CAP, D), jnp.bfloat16).at[expert_of, slot_of].set(h_two[source_rows])

    def run_expert(packed):
        inputs_here, gate_here, up_here, down_here = packed
        gate_pre = jnp.dot(inputs_here, gate_here, preferred_element_type=jnp.float32)
        up_pre = jnp.dot(inputs_here, up_here, preferred_element_type=jnp.float32)
        hidden = (jax.nn.silu(gate_pre) * up_pre).astype(jnp.bfloat16)
        return split_sum(hidden, down_here).astype(jnp.bfloat16)
    expert_rows = lax.map(run_expert, (buffer, expert_gate, expert_up, expert_down))
    picked = expert_rows[expert_of, slot_of].astype(jnp.float32).reshape(SEQUENCE_TOTAL, TOP, D)
    routed_sum = lax.optimization_barrier(jnp.sum(picked * route_weight[:, :, None], axis=1))
    dense_pre = jnp.dot(h_two, dense_gate, preferred_element_type=jnp.float32)
    dense_lift = jnp.dot(h_two, dense_up, preferred_element_type=jnp.float32)
    dense_act = (jax.nn.silu(dense_pre) * dense_lift).astype(jnp.bfloat16)
    dense_out = split_sum(dense_act, dense_down)
    blend_gate = jax.nn.sigmoid(jnp.dot(h_two, mix_gate, preferred_element_type=jnp.float32))
    return (residual.astype(jnp.float32) + routed_sum + blend_gate[:, None] * dense_out).astype(jnp.bfloat16)
```

```python
import jax
import jax.numpy as jnp
from jax import lax
from jax.experimental import pallas as pl
from jax.experimental.pallas import tpu as pltpu
from jax.sharding import PartitionSpec as P

EPS = 1e-06
F32 = jnp.float32
BF16 = jnp.bfloat16
MESH = pl.DeviceIdType.MESH
ANY = pl.ANY

TOK = 16
HD = 64
NTP = 4
NZ = 8
NR = 8
NEP = 64
W = 512
NT = (((1,), (1,)), ((), ()))


def iota(shape, dim):
    return lax.broadcasted_iota(jnp.int32, shape, dim)


def dot(a, b):
    return jnp.dot(a, b, preferred_element_type=F32)


def dot_nt(a, b):
    return lax.dot_general(a, b, NT, preferred_element_type=F32)


def one_hot(mask):
    return jnp.where(mask, 1.0, 0.0).astype(BF16)


def three_parts(a):
    hi = a.astype(BF16)
    rest = a - hi.astype(F32)
    mid = rest.astype(BF16)
    low = (rest - mid.astype(F32)).astype(BF16)
    return hi, mid, low


def gain_row(gain_ref):
    gain = gain_ref[...].astype(F32)
    return jnp.concatenate([gain[j : j + 1, :] for j in range(16)], axis=1)


def silu(a):
    return a * (1.0 / (1.0 + jnp.exp(-a)))


def layer(
    tokens,
    lengths,
    forget_bias,
    attn_gain,
    ffn_gain,
    mix_gate,
    chosen,
    route_weight,
    kv_hbm,
    cum_hbm,
    wq_hbm,
    wk_hbm,
    wv_hbm,
    wf_hbm,
    wo_hbm,
    eg_hbm,
    eu_hbm,
    ed_hbm,
    dg_hbm,
    du_hbm,
    dd_hbm,
    out,
    kv,
    cum,
    wq,
    wkv,
    wf,
    wo,
    eg,
    eu,
    ed,
    dg,
    du,
    dd,
    xbuf,
    gate,
    q2,
    sc,
    ob,
    pbuf,
    abuf,
    dmat,
    rmat,
    perm,
    permt,
    resb,
    rbuf,
    outg,
    gath,
    hbuf,
    dsend,
    dbuf,
    ysend,
    ybuf,
    rout,
    rin,
    ffn32,
    load_sem,
    kv_sem,
    x_send,
    x_recv,
    ready_a,
    ready_b,
    p_send,
    p_recv,
    r_send,
    r_recv,
    o_send,
    o_recv,
    g_send,
    g_recv,
    d_send,
    d_recv,
    y_send,
    y_recv,
    b_send,
    b_recv,
):
    ep = lax.axis_index("ep")
    tp = lax.axis_index("tp")
    z = ep // NR
    r = ep % NR
    peers = [(tp + i) % NTP for i in (2, 1, 3)]

    def load(src, dst, i):
        copy = pltpu.make_async_copy(src, dst, load_sem.at[i])
        copy.start()
        return copy

    def remote(src, dst, send, recv, device):
        return pltpu.make_async_remote_copy(
            src_ref=src,
            dst_ref=dst,
            send_sem=send,
            recv_sem=recv,
            device_id=device,
            device_id_type=MESH,
        )

    def arrived(ref, sem):
        remote(ref, ref, x_send, sem, {"tp": peers[0]}).wait_recv()

    def left(ref, sem):
        remote(ref, ref, sem, x_recv.at[0], {"tp": peers[0]}).wait_send()

    barrier = pltpu.get_barrier_semaphore()
    for p in peers:
        pl.semaphore_signal(barrier, inc=1, device_id={"tp": p}, device_id_type=MESH)
    for i in range(1, NR):
        pl.semaphore_signal(
            barrier, inc=1, device_id={"ep": z * NR + (r + i) % NR}, device_id_type=MESH
        )
    for i in (1, 2, 6, 7):
        pl.semaphore_signal(
            barrier, inc=1, device_id={"ep": ((z + i) % NZ) * NR + r}, device_id_type=MESH
        )

    loads = {}
    loads["cum"] = load(cum_hbm, cum, 0)
    loads["wk"] = load(wk_hbm, wkv.at[pl.ds(0, 64)], 1)
    loads["wv"] = load(wv_hbm, wkv.at[pl.ds(64, 64)], 2)
    loads["wf"] = load(wf_hbm, wf, 3)
    loads["wq"] = load(wq_hbm, wq, 4)
    kv_loads = []
    for p in range(8):
        copy = pltpu.make_async_copy(
            kv_hbm.at[pl.ds(2 * p, 2)], kv.at[pl.ds(2 * p, 2)], kv_sem.at[p]
        )
        copy.start()
        kv_loads.append(copy)
    loads["wo"] = load(wo_hbm, wo, 5)
    loads["dg"] = load(dg_hbm, dg, 6)
    loads["du"] = load(du_hbm, du, 7)
    loads["dd"] = load(dd_hbm, dd, 8)
    loads["eg"] = load(eg_hbm, eg, 9)
    loads["eu"] = load(eu_hbm, eu, 10)
    loads["ed"] = load(ed_hbm, ed, 11)

    pl.semaphore_wait(barrier, 14)

    for p in peers:
        remote(tokens, xbuf.at[tp], x_send, x_recv.at[tp], {"tp": p}).start()
    for i in (2, 6):
        pl.semaphore_signal(
            ready_a, inc=1, device_id={"ep": ((z + i) % NZ) * NR + r}, device_id_type=MESH
        )
    xbuf[tp] = tokens[...]
    ffn32[...] = ffn_gain[...].astype(F32)

    loads["cum"].wait()

    def gate_pair(p, carry):
        both = jnp.concatenate([cum[2 * p], cum[2 * p + 1]], axis=0)
        row = iota((8, 1024), 0)
        pos = iota((8, 1024), 1)
        length = jnp.where(row < 4, lengths[2 * p], lengths[2 * p + 1])
        last = jnp.sum(jnp.where(pos == length - 1, both, 0.0), axis=1, keepdims=True)
        gate[pl.ds(pl.multiple_of(8 * p, 8), 8), :] = jnp.where(
            pos < length, last - both, -jnp.inf
        )
        return carry

    lax.fori_loop(0, 8, gate_pair, 0)

    pl.semaphore_wait(ready_a, 2)
    for i in range(1, NR):
        pl.semaphore_signal(
            ready_b, inc=1, device_id={"ep": z * NR + (r + i) % NR}, device_id_type=MESH
        )

    pick = chosen[...]
    expert = iota((NEP, TOK), 0)
    hot = [jnp.where(expert == pick[k : k + 1, :], 1.0, 0.0) for k in range(2)]
    earlier = one_hot(iota((TOK, TOK), 0) < iota((TOK, TOK), 1))
    before = dot((hot[0] + hot[1]).astype(BF16), earlier)
    slots = [
        2.0 * pick[k : k + 1, :].astype(F32) + jnp.sum(hot[k] * before, axis=0, keepdims=True)
        for k in range(2)
    ]
    weight = route_weight[...]
    w_rows = [three_parts(weight[k : k + 1, :]) for k in range(2)]
    info = jnp.concatenate(
        slots + [part.astype(F32) for k in range(2) for part in w_rows[k]], axis=0
    ).astype(BF16)
    spread = one_hot(iota((TOK, 64), 0) == iota((TOK, 64), 1) % TOK)
    spread_t = one_hot(iota((64, TOK), 0) % TOK == iota((64, TOK), 1))
    info_rows = dot(info, spread).astype(jnp.int32)
    info_cols = dot_nt(spread_t, info)
    row = iota((512, 64), 0)
    col_fb = iota((512, 64), 1) // TOK
    dmask = jnp.zeros((512, 64), F32)
    for k in range(2):
        dmask = dmask + jnp.where(row == info_rows[k : k + 1, :] * 4 + col_fb, 1.0, 0.0)
    dmat[...] = dmask.astype(BF16)
    lane = iota((64, 512), 1)
    row_fb = iota((64, 512), 0) // TOK
    for k in range(2):
        slot_col = info_cols[:, k : k + 1].astype(jnp.int32)
        rmat[pl.ds(64 * k, 64), :] = one_hot(lane == slot_col * 4 + row_fb)
    w_cols = [
        info_cols[:, 2 + 3 * k : 3 + 3 * k]
        + info_cols[:, 3 + 3 * k : 4 + 3 * k]
        + info_cols[:, 4 + 3 * k : 5 + 3 * k]
        for k in range(2)
    ]

    def perm_part(i, carry):
        base = pl.multiple_of(64 * i, 64)
        a = iota((64, 512), 0) + base
        b = iota((64, 512), 1)
        perm[pl.ds(base, 64), :] = one_hot((a % 128) * 4 + a // 128 == b)
        permt[pl.ds(base, 64), :] = one_hot((b % 128) * 4 + b // 128 == a)
        return carry

    lax.fori_loop(0, 8, perm_part, 0)

    for p in peers:
        arrived(xbuf.at[p], x_recv.at[p])
    x_full = jnp.concatenate([xbuf[p] for p in range(NTP)], axis=1).astype(F32)
    square = jnp.mean(x_full * x_full, axis=1, keepdims=True)
    h_one = (x_full * lax.rsqrt(square + EPS) * gain_row(attn_gain)).astype(BF16)

    for name in ("wk", "wv", "wf", "wq"):
        loads[name].wait()
    query = dot(h_one, wq[...]).astype(BF16)
    kv_new = dot_nt(h_one, wkv[...]).astype(BF16)
    forget = dot_nt(h_one, wf[...])
    head_lane = iota((TOK, 4), 1)
    bias = jnp.zeros((TOK, 4), F32)
    for h in range(4):
        bias = jnp.where(head_lane == h, forget_bias[h], bias)
    forget = forget + bias
    forget = jnp.minimum(forget, 0.0) - jnp.log1p(jnp.exp(-jnp.abs(forget)))

    row64 = iota((64, TOK), 0)
    col16 = iota((64, TOK), 1)
    repeat = one_hot(row64 // 4 == col16)
    row32 = iota((64, 32), 0)
    col32 = iota((64, 32), 1)
    even = one_hot((row32 // 4 == col32 % TOK) & (row32 % 4 == (col32 // TOK) * 2))
    odd = one_hot((row32 // 4 == col32 % TOK) & (row32 % 4 == (col32 // TOK) * 2 + 1))
    stacked = jnp.concatenate([query[:, 0:128], query[:, 128:256]], axis=0)
    low_half = iota((64, 128), 1) < HD
    q64 = jnp.where(
        low_half, dot(even, stacked) + pltpu.roll(dot(odd, stacked), HD, 1), 0.0
    )
    kv64 = dot(repeat, kv_new)
    f_parts = three_parts(forget)
    f64 = dot(repeat, f_parts[0]) + dot(repeat, f_parts[1]) + dot(repeat, f_parts[2])
    f64 = jnp.sum(
        jnp.where(iota((64, 4), 0) % 4 == iota((64, 4), 1), f64, 0.0), axis=1, keepdims=True
    )
    scale = HD ** (-0.5)
    own = jnp.sum(q64 * kv64, axis=1, keepdims=True) * scale - f64
    first = iota((64, 128), 0) % 8 < 4
    q2[:, 0:128] = jnp.where(first, q64, 0.0)
    q2[:, 128:256] = jnp.where(first, 0.0, q64)

    for p in range(8):
        kv_loads[p].wait()
        keys = jnp.concatenate([kv[2 * p], kv[2 * p + 1]], axis=1)
        sc[pl.ds(8 * p, 8), :] = dot_nt(q2[pl.ds(8 * p, 8), :].astype(BF16), keys)
    score = sc[...] * scale + gate[...]
    highest = jnp.maximum(jnp.max(score, axis=1, keepdims=True), own)
    prob = jnp.exp(score - highest)
    own_prob = jnp.exp(own - highest)
    total = jnp.sum(prob, axis=1, keepdims=True) + own_prob
    inverse = 1.0 / total
    sc[...] = prob * inverse
    own_prob = own_prob * inverse
    for p in range(8):
        values = jnp.concatenate([kv[2 * p], kv[2 * p + 1]], axis=1)
        ob[pl.ds(8 * p, 8), :] = dot(sc[pl.ds(8 * p, 8), :].astype(BF16), values)
    blended = jnp.where(first, ob[:, 0:128], ob[:, 128:256])
    blended = (blended + own_prob.astype(BF16).astype(F32) * kv64).astype(BF16)
    back = one_hot(
        iota((64, 64), 1) == (iota((64, 64), 0) % TOK) * 4 + iota((64, 64), 0) // TOK
    )
    heads = dot(back, blended)
    low16 = iota((TOK, 128), 1) < HD
    head_out = jnp.concatenate(
        [
            jnp.where(low16, pltpu.roll(heads[0:16], HD, 1), heads[16:32]),
            jnp.where(low16, pltpu.roll(heads[32:48], HD, 1), heads[48:64]),
        ],
        axis=1,
    ).astype(BF16)
    loads["wo"].wait()
    partial = dot(head_out, wo[...]).astype(BF16)
    for p in range(NTP):
        pbuf[p] = partial[:, p * W : (p + 1) * W]
    for p in peers:
        remote(pbuf.at[p], abuf.at[tp], p_send, p_recv.at[tp], {"tp": p}).start()
    abuf[tp] = pbuf[tp]

    pl.semaphore_wait(ready_b, 7)

    for p in peers:
        arrived(abuf.at[p], p_recv.at[p])
    attention = abuf[0].astype(F32)
    for p in range(1, NTP):
        attention = attention + abuf[p].astype(F32)
    residual = (tokens[...].astype(F32) + attention).astype(BF16)
    resb[...] = residual
    stacked = jnp.concatenate([residual[:, f * 128 : (f + 1) * 128] for f in range(4)], axis=0)
    outgoing = dot(dmat[...], stacked)
    outg[...] = outgoing.reshape(NEP, 8, 128).astype(BF16)

    def send_out(i, carry):
        k = i // NR
        dz = jnp.where(k % 2 == 1, 4 - (k + 1) // 2, (4 + k // 2) % 8)
        dr = (r + i + 1) % NR
        e = ((z + dz) % NZ) * NR + dr
        remote(outg.at[e], gath.at[tp, ep], o_send, o_recv.at[z], {"ep": e}).start()
        return carry

    lax.fori_loop(0, 63, send_out, 0)
    gath[tp, ep] = outg[ep]
    for p in peers:
        remote(resb, rbuf.at[tp], r_send, r_recv.at[tp], {"tp": p}).start()
    rbuf[tp] = resb[...]

    for dz in (0, 1, 7, 2, 6, 3, 5, 4):
        src_z = (z + dz) % NZ
        base = src_z * NR
        count = NR - 1 if dz == 0 else NR
        arrived(gath.at[tp, pl.ds(base, count)], o_recv.at[src_z])
        chunk = gath.at[tp, pl.ds(base, NR)]
        for p in peers:
            remote(chunk, chunk, g_send, g_recv.at[tp], {"tp": p}).start()

    for p in peers:
        arrived(rbuf.at[p], r_recv.at[p])
    res_full = jnp.concatenate([rbuf[p] for p in range(NTP)], axis=1).astype(F32)
    square = jnp.mean(res_full * res_full, axis=1, keepdims=True)
    ffn_row = gain_row(ffn_gain)
    h_two = (res_full * lax.rsqrt(square + EPS) * ffn_row).astype(BF16)
    for name in ("dg", "du", "dd"):
        loads[name].wait()
    dense_act = (silu(dot(h_two, dg[...])) * dot(h_two, du[...])).astype(BF16)
    dense_part = dot(dense_act, dd[...]).astype(BF16)
    for p in range(NTP):
        dsend[p] = dense_part[:, p * W : (p + 1) * W]
    for p in peers:
        remote(dsend.at[p], dbuf.at[tp], d_send, d_recv.at[tp], {"tp": p}).start()
    dbuf[tp] = dsend[tp]
    mixing = jnp.sum(h_two.astype(F32) * gain_row(mix_gate), axis=1, keepdims=True)
    blend = 1.0 / (1.0 + jnp.exp(-mixing))

    for name in ("eg", "eu", "ed"):
        loads[name].wait()
    squares = jnp.zeros((128, 128), F32)
    for i in (0, 1, 3, 2):
        p = (tp + i) % NTP
        if i:
            arrived(gath.at[p], g_recv.at[p])
        rows = dot(perm[...], gath[p].reshape(512, 128))
        for f in range(4):
            block = rows[128 * f : 128 * f + 128]
            squares = squares + block * block
            c = p * 4 + f
            scaled = block * ffn32[pl.ds(c, 1), :]
            hbuf[:, pl.ds(pl.multiple_of(c * 128, 128), 128)] = scaled.astype(BF16)
    root = lax.rsqrt(jnp.sum(squares, axis=1, keepdims=True) * (1.0 / 2048.0) + EPS)
    hidden = hbuf[...]
    gate_pre = dot(hidden, eg[...]) * root
    up_pre = dot(hidden, eu[...]) * root
    act = (silu(gate_pre) * up_pre).astype(BF16)
    for p in peers:
        ysend[p] = dot(act, ed[:, pl.ds(pl.multiple_of(p * W, W), W)]).astype(BF16)
        remote(ysend.at[p], ybuf.at[tp], y_send, y_recv.at[tp], {"tp": p}).start()
    summed = dot(act, ed[:, pl.ds(pl.multiple_of(tp * W, W), W)]).astype(BF16).astype(F32)
    for p in peers:
        arrived(ybuf.at[p], y_recv.at[p])
        summed = summed + ybuf[p].astype(F32)
    summed = summed.astype(BF16)
    stacked = jnp.concatenate([summed[:, f * 128 : (f + 1) * 128] for f in range(4)], axis=0)
    rout[...] = dot(permt[...], stacked).reshape(NEP, 8, 128).astype(BF16)

    def send_back(i, carry):
        k = i // NR
        dz = jnp.where(k % 2 == 1, 4 - (k + 1) // 2, (4 + k // 2) % 8)
        dr = (r + i + 1) % NR
        e = ((z + dz) % NZ) * NR + dr
        remote(rout.at[e], rin.at[ep], b_send, b_recv, {"ep": e}).start()
        return carry

    lax.fori_loop(0, 63, send_back, 0)
    rin[ep] = rout[ep]

    for p in peers:
        arrived(dbuf.at[p], d_recv.at[p])
    dense_out = dbuf[0].astype(F32)
    for p in range(1, NTP):
        dense_out = dense_out + dbuf[p].astype(F32)
    mixed = residual.astype(F32) + blend * dense_out

    arrived(rin.at[pl.ds(0, 63)], b_recv)
    picked = dot(rmat[...], rin[...].reshape(512, 128))
    routed = picked[0:64] * w_cols[0] + picked[64:128] * w_cols[1]
    routed = jnp.concatenate([routed[16 * f : 16 * f + 16] for f in range(4)], axis=1)
    out[...] = (mixed + routed).astype(BF16)

    left(xbuf.at[pl.ds(0, 3)], x_send)
    left(pbuf.at[pl.ds(0, 3)], p_send)
    left(rbuf.at[pl.ds(0, 3)], r_send)
    left(outg.at[pl.ds(0, 63)], o_send)
    left(gath.at[pl.ds(0, 3)], g_send)
    left(dsend.at[pl.ds(0, 3)], d_send)
    left(ysend.at[pl.ds(0, 3)], y_send)
    left(rout.at[pl.ds(0, 63)], b_send)


def local(
    tokens,
    kv_cache,
    cum_gate,
    lengths,
    w_query,
    w_key,
    w_value,
    w_forget,
    forget_bias,
    w_out,
    attn_gain,
    ffn_gain,
    mix_gate,
    expert_gate,
    expert_up,
    expert_down,
    chosen,
    route_weight,
    dense_gate,
    dense_up,
    dense_down,
):
    smem = pl.BlockSpec(memory_space=pltpu.SMEM)
    vmem = pl.BlockSpec(memory_space=pltpu.VMEM)
    hbm = pl.BlockSpec(memory_space=ANY)
    dma = pltpu.SemaphoreType.DMA
    regular = pltpu.SemaphoreType.REGULAR
    scratch = [
        pltpu.VMEM((TOK, 1024, 128), BF16),
        pltpu.VMEM((TOK, 4, 1024), F32),
        pltpu.VMEM((2048, 256), BF16),
        pltpu.VMEM((128, 2048), BF16),
        pltpu.VMEM((4, 2048), BF16),
        pltpu.VMEM((256, 2048), BF16),
        pltpu.VMEM((2048, 256), BF16),
        pltpu.VMEM((2048, 256), BF16),
        pltpu.VMEM((256, 2048), BF16),
        pltpu.VMEM((2048, 256), BF16),
        pltpu.VMEM((2048, 256), BF16),
        pltpu.VMEM((256, 2048), BF16),
        pltpu.VMEM((NTP, TOK, W), BF16),
        pltpu.VMEM((64, 1024), F32),
        pltpu.VMEM((64, 256), F32),
        pltpu.VMEM((64, 1024), F32),
        pltpu.VMEM((64, 256), F32),
        pltpu.VMEM((NTP, TOK, W), BF16),
        pltpu.VMEM((NTP, TOK, W), BF16),
        pltpu.VMEM((512, 64), BF16),
        pltpu.VMEM((128, 512), BF16),
        pltpu.VMEM((512, 512), BF16),
        pltpu.VMEM((512, 512), BF16),
        pltpu.VMEM((TOK, W), BF16),
        pltpu.VMEM((NTP, TOK, W), BF16),
        pltpu.VMEM((NEP, 8, 128), BF16),
        pltpu.VMEM((NTP, NEP, 8, 128), BF16),
        pltpu.VMEM((128, 2048), BF16),
        pltpu.VMEM((NTP, TOK, W), BF16),
        pltpu.VMEM((NTP, TOK, W), BF16),
        pltpu.VMEM((NTP, 128, W), BF16),
        pltpu.VMEM((NTP, 128, W), BF16),
        pltpu.VMEM((NEP, 8, 128), BF16),
        pltpu.VMEM((NEP, 8, 128), BF16),
        pltpu.VMEM((16, 128), F32),
        dma((12,)),
        dma((8,)),
        dma,
        dma((NTP,)),
        regular,
        regular,
        dma,
        dma((NTP,)),
        dma,
        dma((NTP,)),
        dma,
        dma((NZ,)),
        dma,
        dma((NTP,)),
        dma,
        dma((NTP,)),
        dma,
        dma((NTP,)),
        dma,
        dma,
    ]
    return pl.pallas_call(
        layer,
        out_shape=jax.ShapeDtypeStruct((TOK, W), BF16),
        in_specs=[vmem, smem, smem, vmem, vmem, vmem, vmem, vmem] + [hbm] * 13,
        out_specs=vmem,
        scratch_shapes=scratch,
        compiler_params=pltpu.CompilerParams(collective_id=0, has_side_effects=True),
        name="layer",
    )(
        tokens,
        lengths,
        forget_bias,
        attn_gain.reshape(16, 128),
        ffn_gain.reshape(16, 128),
        mix_gate.reshape(16, 128),
        chosen.T,
        route_weight.T,
        kv_cache,
        cum_gate,
        w_query,
        w_key.T,
        w_value.T,
        w_forget.T,
        w_out,
        expert_gate[0],
        expert_up[0],
        expert_down[0],
        dense_gate,
        dense_up,
        dense_down,
    )


def solution(mesh):
    in_specs = (
        P("ep", "tp"),
        P("ep", None, "tp"),
        P("ep", "tp", None),
        P("ep"),
        P(None, "tp"),
        P(None, "tp"),
        P(None, "tp"),
        P(None, "tp"),
        P("tp"),
        P("tp", None),
        P(),
        P(),
        P(),
        P("ep", None, "tp"),
        P("ep", None, "tp"),
        P("ep", "tp", None),
        P("ep", None),
        P("ep", None),
        P(None, "tp"),
        P(None, "tp"),
        P("tp", None),
    )
    out_specs = P("ep", "tp")
    return jax.shard_map(local, mesh=mesh, in_specs=in_specs, out_specs=out_specs, check_vma=False)
```

```python
import jax
import jax.numpy as jnp
from jax import lax
from jax.experimental import pallas as pl
from jax.experimental.pallas import tpu as pltpu
from jax.sharding import PartitionSpec as P

EPS = 1e-06
F32 = jnp.float32
BF16 = jnp.bfloat16
MESH = pl.DeviceIdType.MESH
ANY = pl.ANY

TOK = 16
HD = 64
NTP = 4
NZ = 8
NR = 8
NEP = 64
W = 512
NT = (((1,), (1,)), ((), ()))


def iota(shape, dim):
    return lax.broadcasted_iota(jnp.int32, shape, dim)


def dot(a, b):
    return jnp.dot(a, b, preferred_element_type=F32)


def dot_nt(a, b):
    return lax.dot_general(a, b, NT, preferred_element_type=F32)


def one_hot(mask):
    return jnp.where(mask, 1.0, 0.0).astype(BF16)


def three_parts(a):
    hi = a.astype(BF16)
    rest = a - hi.astype(F32)
    mid = rest.astype(BF16)
    low = (rest - mid.astype(F32)).astype(BF16)
    return hi, mid, low


def gain_row(gain_ref):
    gain = gain_ref[...].astype(F32)
    return jnp.concatenate([gain[j : j + 1, :] for j in range(16)], axis=1)


def silu(a):
    return a * (1.0 / (1.0 + jnp.exp(-a)))


def layer(
    tokens_hbm,
    lengths_hbm,
    bias_hbm,
    attn_hbm,
    ffn_hbm,
    mix_hbm,
    chosen_hbm,
    route_hbm,
    kv_hbm,
    cum_hbm,
    wq_hbm,
    wk_hbm,
    wv_hbm,
    wf_hbm,
    wo_hbm,
    eg_hbm,
    eu_hbm,
    ed_hbm,
    dg_hbm,
    du_hbm,
    dd_hbm,
    out,
    tokens,
    lengths,
    forget_bias,
    attn_gain,
    ffn_gain,
    mix_gate,
    chosen,
    route_weight,
    kv,
    keys,
    cum,
    wq,
    wkv,
    wf,
    wo,
    eg,
    eu,
    ed,
    dg,
    du,
    dd,
    xbuf,
    gate,
    sc,
    ob,
    pbuf,
    abuf,
    dmat,
    rmat,
    perm,
    permt,
    resb,
    rbuf,
    outg,
    gath,
    hbuf,
    dsend,
    dbuf,
    ysend,
    ybuf,
    rout,
    rin,
    ffn32,
    load_sem,
    kv_sem,
    x_send,
    x_recv,
    ready_a,
    ready_b,
    p_send,
    p_recv,
    r_send,
    r_recv,
    o_send,
    o_recv,
    g_send,
    g_recv,
    d_send,
    d_recv,
    y_send,
    y_recv,
    b_send,
    b_recv,
):
    ep = lax.axis_index("ep")
    tp = lax.axis_index("tp")
    z = ep // NR
    r = lax.rem(ep, NR)
    peers = [lax.rem(tp + i, NTP) for i in (2, 1, 3)]
    planes = [lax.rem(z + i, NZ) for i in range(NZ)]
    mates = [lax.rem(r + i, NR) for i in range(NR)]
    order = (0, 1, 7, 2, 6, 3, 5, 4)

    def load(src, dst, i):
        copy = pltpu.make_async_copy(src, dst, load_sem.at[i])
        copy.start()
        return copy

    def remote(src, dst, send, recv, device):
        return pltpu.make_async_remote_copy(
            src_ref=src,
            dst_ref=dst,
            send_sem=send,
            recv_sem=recv,
            device_id=device,
            device_id_type=MESH,
        )

    def arrived(ref, sem):
        remote(ref, ref, x_send, sem, {"tp": peers[0]}).wait_recv()

    def left(ref, sem):
        remote(ref, ref, sem, x_recv.at[0], {"tp": peers[0]}).wait_send()

    barrier = pltpu.get_barrier_semaphore()
    for p in peers:
        pl.semaphore_signal(barrier, inc=1, device_id={"tp": p}, device_id_type=MESH)
    for i in range(1, NR):
        pl.semaphore_signal(
            barrier, inc=1, device_id={"ep": z * NR + mates[i]}, device_id_type=MESH
        )
    for i in (1, 2, 6, 7):
        pl.semaphore_signal(
            barrier, inc=1, device_id={"ep": planes[i] * NR + r}, device_id_type=MESH
        )

    loads = {}
    loads["tokens"] = load(tokens_hbm, tokens, 12)
    loads["lengths"] = load(lengths_hbm, lengths, 13)
    loads["cum"] = load(cum_hbm, cum, 0)
    loads["chosen"] = load(chosen_hbm, chosen, 14)
    loads["route"] = load(route_hbm, route_weight, 15)
    loads["attn"] = load(attn_hbm, attn_gain, 16)
    loads["ffn"] = load(ffn_hbm, ffn_gain, 17)
    loads["mix"] = load(mix_hbm, mix_gate, 18)
    loads["bias"] = load(bias_hbm, forget_bias, 19)

    def kv_load(q):
        part = pl.ds(4 * q, 4)
        return pltpu.make_async_copy(kv_hbm.at[part], kv.at[part], kv_sem.at[q])

    for q in range(4):
        kv_load(q).start()
    loads["wk"] = load(wk_hbm, wkv.at[pl.ds(0, 64)], 1)
    loads["wv"] = load(wv_hbm, wkv.at[pl.ds(64, 64)], 2)
    loads["wf"] = load(wf_hbm, wf, 3)
    loads["wq"] = load(wq_hbm, wq, 4)
    loads["wo"] = load(wo_hbm, wo, 5)
    loads["dg"] = load(dg_hbm, dg, 6)
    loads["du"] = load(du_hbm, du, 7)
    loads["dd"] = load(dd_hbm, dd, 8)
    loads["eg"] = load(eg_hbm, eg, 9)
    loads["eu"] = load(eu_hbm, eu, 10)
    loads["ed"] = load(ed_hbm, ed, 11)

    loads["tokens"].wait()
    pl.semaphore_wait(barrier, 14)

    for p in peers:
        remote(tokens, xbuf.at[tp], x_send, x_recv.at[tp], {"tp": p}).start()
    for i in (2, 6):
        pl.semaphore_signal(
            ready_a, inc=1, device_id={"ep": planes[i] * NR + r}, device_id_type=MESH
        )
    xbuf[tp] = tokens[...]

    for name in ("lengths", "cum"):
        loads[name].wait()

    def gate_pair(p, carry):
        both = jnp.concatenate([cum[2 * p], cum[2 * p + 1]], axis=0)
        row = iota((8, 1024), 0)
        pos = iota((8, 1024), 1)
        length = jnp.where(row < 4, lengths[2 * p], lengths[2 * p + 1])
        last = jnp.sum(jnp.where(pos == length - 1, both, 0.0), axis=1, keepdims=True)
        gate[pl.ds(pl.multiple_of(8 * p, 8), 8), :] = jnp.where(
            pos < length, last - both, -jnp.inf
        )
        return carry

    lax.fori_loop(0, 8, gate_pair, 0)

    for name in ("chosen", "route"):
        loads[name].wait()
    pick = chosen[...]
    expert = iota((NEP, TOK), 0)
    hot = [jnp.where(expert == pick[k : k + 1, :], 1.0, 0.0) for k in range(2)]
    earlier = one_hot(iota((TOK, TOK), 0) < iota((TOK, TOK), 1))
    before = dot((hot[0] + hot[1]).astype(BF16), earlier)
    slots = [
        2.0 * pick[k : k + 1, :].astype(F32) + jnp.sum(hot[k] * before, axis=0, keepdims=True)
        for k in range(2)
    ]
    weight = route_weight[...]
    w_rows = [three_parts(weight[k : k + 1, :]) for k in range(2)]
    info = jnp.concatenate(
        slots + [part.astype(F32) for k in range(2) for part in w_rows[k]], axis=0
    ).astype(BF16)
    spread = one_hot(iota((TOK, 64), 0) == iota((TOK, 64), 1) % TOK)
    spread_t = one_hot(iota((64, TOK), 0) % TOK == iota((64, TOK), 1))
    info_rows = dot(info, spread).astype(jnp.int32)
    info_cols = dot_nt(spread_t, info)
    row = iota((512, 64), 0)
    col_fb = iota((512, 64), 1) // TOK
    dmask = jnp.zeros((512, 64), F32)
    for k in range(2):
        dmask = dmask + jnp.where(row == info_rows[k : k + 1, :] * 4 + col_fb, 1.0, 0.0)
    dmat[...] = dmask.astype(BF16)
    lane = iota((64, 512), 1)
    row_fb = iota((64, 512), 0) // TOK
    for k in range(2):
        slot_col = info_cols[:, k : k + 1].astype(jnp.int32)
        rmat[pl.ds(64 * k, 64), :] = one_hot(lane == slot_col * 4 + row_fb)
    w_cols = [
        info_cols[:, 2 + 3 * k : 3 + 3 * k]
        + info_cols[:, 3 + 3 * k : 4 + 3 * k]
        + info_cols[:, 4 + 3 * k : 5 + 3 * k]
        for k in range(2)
    ]

    def key_part(q, carry):
        kv_load(q).wait()
        for i in range(4):
            turned = jnp.transpose(kv[4 * q + i])
            keys[q, 64 * i : 64 * i + 64, :] = turned[0:64]
        return carry

    lax.fori_loop(0, 4, key_part, 0)

    pl.semaphore_wait(ready_a, 2)
    for i in range(1, NR):
        pl.semaphore_signal(
            ready_b, inc=1, device_id={"ep": z * NR + mates[i]}, device_id_type=MESH
        )

    for name in ("attn", "bias"):
        loads[name].wait()
    for p in peers:
        arrived(xbuf.at[p], x_recv.at[p])
    x_full = jnp.concatenate([xbuf[p] for p in range(NTP)], axis=1).astype(F32)
    square = jnp.mean(x_full * x_full, axis=1, keepdims=True)
    h_one = (x_full * lax.rsqrt(square + EPS) * gain_row(attn_gain)).astype(BF16)

    for name in ("wk", "wv", "wf", "wq"):
        loads[name].wait()
    query = dot(h_one, wq[...]).astype(BF16)
    kv_new = dot_nt(h_one, wkv[...]).astype(BF16)
    forget = dot_nt(h_one, wf[...])
    head_lane = iota((TOK, 4), 1)
    bias = jnp.zeros((TOK, 4), F32)
    for h in range(4):
        bias = jnp.where(head_lane == h, forget_bias[h], bias)
    forget = forget + bias
    forget = jnp.minimum(forget, 0.0) - jnp.log1p(jnp.exp(-jnp.abs(forget)))

    row64 = iota((64, TOK), 0)
    col16 = iota((64, TOK), 1)
    repeat = one_hot(row64 // 4 == col16)
    row32 = iota((64, 32), 0)
    col32 = iota((64, 32), 1)
    even = one_hot((row32 // 4 == col32 % TOK) & (row32 % 4 == (col32 // TOK) * 2))
    odd = one_hot((row32 // 4 == col32 % TOK) & (row32 % 4 == (col32 // TOK) * 2 + 1))
    stacked = jnp.concatenate([query[:, 0:128], query[:, 128:256]], axis=0)
    low_half = iota((64, 128), 1) < HD
    q64 = jnp.where(
        low_half, dot(even, stacked) + pltpu.roll(dot(odd, stacked), HD, 1), 0.0
    )
    kv64 = dot(repeat, kv_new)
    f_parts = three_parts(forget)
    f64 = dot(repeat, f_parts[0]) + dot(repeat, f_parts[1]) + dot(repeat, f_parts[2])
    f64 = jnp.sum(
        jnp.where(iota((64, 4), 0) % 4 == iota((64, 4), 1), f64, 0.0), axis=1, keepdims=True
    )
    scale = HD ** (-0.5)
    own = jnp.sum(q64 * kv64, axis=1, keepdims=True) * scale - f64
    first = iota((64, 128), 0) % 8 < 4
    wide = jnp.concatenate([q64, q64], axis=1)
    wide = wide + pltpu.roll(wide, HD, 1)
    own_lanes = (iota((64, 256), 0) // 4) % 4 == iota((64, 256), 1) // HD
    blocks = jnp.where(own_lanes, wide, 0.0).astype(BF16)
    for q in range(4):
        sc[pl.ds(16 * q, 16), :] = dot(blocks[16 * q : 16 * q + 16], keys[q])
    score = sc[...] * scale + gate[...]
    highest = jnp.maximum(jnp.max(score, axis=1, keepdims=True), own)
    prob = jnp.exp(score - highest)
    own_prob = jnp.exp(own - highest)
    total = jnp.sum(prob, axis=1, keepdims=True) + own_prob
    inverse = 1.0 / total
    sc[...] = prob * inverse
    own_prob = own_prob * inverse
    for p in range(8):
        values = jnp.concatenate([kv[2 * p], kv[2 * p + 1]], axis=1)
        ob[pl.ds(8 * p, 8), :] = dot(sc[pl.ds(8 * p, 8), :].astype(BF16), values)
    blended = jnp.where(first, ob[:, 0:128], ob[:, 128:256])
    blended = (blended + own_prob.astype(BF16).astype(F32) * kv64).astype(BF16)
    back = one_hot(
        iota((64, 64), 1) == (iota((64, 64), 0) % TOK) * 4 + iota((64, 64), 0) // TOK
    )
    heads = dot(back, blended)
    low16 = iota((TOK, 128), 1) < HD
    head_out = jnp.concatenate(
        [
            jnp.where(low16, pltpu.roll(heads[0:16], HD, 1), heads[16:32]),
            jnp.where(low16, pltpu.roll(heads[32:48], HD, 1), heads[48:64]),
        ],
        axis=1,
    ).astype(BF16)
    loads["wo"].wait()
    partial = dot(head_out, wo[...]).astype(BF16)
    for p in range(NTP):
        pbuf[p] = partial[:, p * W : (p + 1) * W]
    for p in peers:
        remote(pbuf.at[p], abuf.at[tp], p_send, p_recv.at[tp], {"tp": p}).start()
    abuf[tp] = pbuf[tp]

    def perm_part(i, carry):
        base = pl.multiple_of(64 * i, 64)
        a = iota((64, 512), 0) + base
        b = iota((64, 512), 1)
        perm[pl.ds(base, 64), :] = one_hot((a % 128) * 4 + a // 128 == b)
        permt[pl.ds(base, 64), :] = one_hot((b % 128) * 4 + b // 128 == a)
        return carry

    lax.fori_loop(0, 8, perm_part, 0)

    for name in ("ffn", "mix"):
        loads[name].wait()
    ffn32[...] = ffn_gain[...].astype(F32)
    pl.semaphore_wait(ready_b, 7)

    for p in peers:
        arrived(abuf.at[p], p_recv.at[p])
    attention = abuf[0].astype(F32)
    for p in range(1, NTP):
        attention = attention + abuf[p].astype(F32)
    residual = (tokens[...].astype(F32) + attention).astype(BF16)
    resb[...] = residual
    stacked = jnp.concatenate([residual[:, f * 128 : (f + 1) * 128] for f in range(4)], axis=0)
    outgoing = dot(dmat[...], stacked)
    outg[...] = outgoing.reshape(NEP, 8, 128).astype(BF16)

    for dz in order:
        for i in range(1, NR + 1):
            if dz or i < NR:
                e = planes[dz] * NR + mates[i % NR]
                remote(outg.at[e], gath.at[tp, ep], o_send, o_recv.at[z], {"ep": e}).start()
    gath[tp, ep] = outg[ep]
    for p in peers:
        remote(resb, rbuf.at[tp], r_send, r_recv.at[tp], {"tp": p}).start()
    rbuf[tp] = resb[...]

    for dz in order:
        src_z = planes[dz]
        base = src_z * NR
        count = NR - 1 if dz == 0 else NR
        arrived(gath.at[tp, pl.ds(base, count)], o_recv.at[src_z])
        chunk = gath.at[tp, pl.ds(base, NR)]
        for p in peers:
            remote(chunk, chunk, g_send, g_recv.at[tp], {"tp": p}).start()

    for p in peers:
        arrived(rbuf.at[p], r_recv.at[p])
    res_full = jnp.concatenate([rbuf[p] for p in range(NTP)], axis=1).astype(F32)
    square = jnp.mean(res_full * res_full, axis=1, keepdims=True)
    ffn_row = gain_row(ffn_gain)
    h_two = (res_full * lax.rsqrt(square + EPS) * ffn_row).astype(BF16)
    for name in ("dg", "du", "dd"):
        loads[name].wait()
    dense_act = (silu(dot(h_two, dg[...])) * dot(h_two, du[...])).astype(BF16)
    dense_part = dot(dense_act, dd[...]).astype(BF16)
    for p in range(NTP):
        dsend[p] = dense_part[:, p * W : (p + 1) * W]
    for p in peers:
        remote(dsend.at[p], dbuf.at[tp], d_send, d_recv.at[tp], {"tp": p}).start()
    dbuf[tp] = dsend[tp]
    mixing = jnp.sum(h_two.astype(F32) * gain_row(mix_gate), axis=1, keepdims=True)
    blend = 1.0 / (1.0 + jnp.exp(-mixing))

    for name in ("eg", "eu", "ed"):
        loads[name].wait()
    squares = jnp.zeros((128, 128), F32)
    for i in (0, 1, 3, 2):
        p = lax.rem(tp + i, NTP)
        if i:
            arrived(gath.at[p], g_recv.at[p])
        rows = dot(perm[...], gath[p].reshape(512, 128))
        for f in range(4):
            block = rows[128 * f : 128 * f + 128]
            squares = squares + block * block
            c = p * 4 + f
            scaled = block * ffn32[pl.ds(c, 1), :]
            hbuf[:, pl.ds(pl.multiple_of(c * 128, 128), 128)] = scaled.astype(BF16)
    root = lax.rsqrt(jnp.sum(squares, axis=1, keepdims=True) * (1.0 / 2048.0) + EPS)
    hidden = hbuf[...]
    gate_pre = dot(hidden, eg[...]) * root
    up_pre = dot(hidden, eu[...]) * root
    act = (silu(gate_pre) * up_pre).astype(BF16)
    for p in peers:
        ysend[p] = dot(act, ed[:, pl.ds(pl.multiple_of(p * W, W), W)]).astype(BF16)
        remote(ysend.at[p], ybuf.at[tp], y_send, y_recv.at[tp], {"tp": p}).start()
    summed = dot(act, ed[:, pl.ds(pl.multiple_of(tp * W, W), W)]).astype(BF16).astype(F32)
    for p in peers:
        arrived(ybuf.at[p], y_recv.at[p])
        summed = summed + ybuf[p].astype(F32)
    summed = summed.astype(BF16)
    stacked = jnp.concatenate([summed[:, f * 128 : (f + 1) * 128] for f in range(4)], axis=0)
    rout[...] = dot(permt[...], stacked).reshape(NEP, 8, 128).astype(BF16)

    for dz in (4, 3, 5, 2, 6, 1, 7, 0):
        for i in range(1, NR + 1):
            if dz or i < NR:
                e = planes[dz] * NR + mates[i % NR]
                remote(rout.at[e], rin.at[ep], b_send, b_recv, {"ep": e}).start()
    rin[ep] = rout[ep]

    for p in peers:
        arrived(dbuf.at[p], d_recv.at[p])
    dense_out = dbuf[0].astype(F32)
    for p in range(1, NTP):
        dense_out = dense_out + dbuf[p].astype(F32)
    mixed = residual.astype(F32) + blend * dense_out

    arrived(rin.at[pl.ds(0, 63)], b_recv)
    picked = dot(rmat[...], rin[...].reshape(512, 128))
    routed = picked[0:64] * w_cols[0] + picked[64:128] * w_cols[1]
    routed = jnp.concatenate([routed[16 * f : 16 * f + 16] for f in range(4)], axis=1)
    out[...] = (mixed + routed).astype(BF16)

    left(xbuf.at[pl.ds(0, 3)], x_send)
    left(pbuf.at[pl.ds(0, 3)], p_send)
    left(rbuf.at[pl.ds(0, 3)], r_send)
    left(outg.at[pl.ds(0, 63)], o_send)
    left(gath.at[pl.ds(0, 3)], g_send)
    left(dsend.at[pl.ds(0, 3)], d_send)
    left(ysend.at[pl.ds(0, 3)], y_send)
    left(rout.at[pl.ds(0, 63)], b_send)


def local(
    tokens,
    kv_cache,
    cum_gate,
    lengths,
    w_query,
    w_key,
    w_value,
    w_forget,
    forget_bias,
    w_out,
    attn_gain,
    ffn_gain,
    mix_gate,
    expert_gate,
    expert_up,
    expert_down,
    chosen,
    route_weight,
    dense_gate,
    dense_up,
    dense_down,
):
    vmem = pl.BlockSpec(memory_space=pltpu.VMEM)
    hbm = pl.BlockSpec(memory_space=ANY)
    dma = pltpu.SemaphoreType.DMA
    regular = pltpu.SemaphoreType.REGULAR
    scratch = [
        pltpu.VMEM((TOK, W), BF16),
        pltpu.SMEM((TOK,), jnp.int32),
        pltpu.SMEM((4,), F32),
        pltpu.VMEM((16, 128), BF16),
        pltpu.VMEM((16, 128), BF16),
        pltpu.VMEM((16, 128), BF16),
        pltpu.VMEM((2, TOK), jnp.int32),
        pltpu.VMEM((2, TOK), F32),
        pltpu.VMEM((TOK, 1024, 128), BF16),
        pltpu.VMEM((4, 256, 1024), BF16),
        pltpu.VMEM((TOK, 4, 1024), F32),
        pltpu.VMEM((2048, 256), BF16),
        pltpu.VMEM((128, 2048), BF16),
        pltpu.VMEM((4, 2048), BF16),
        pltpu.VMEM((256, 2048), BF16),
        pltpu.VMEM((2048, 256), BF16),
        pltpu.VMEM((2048, 256), BF16),
        pltpu.VMEM((256, 2048), BF16),
        pltpu.VMEM((2048, 256), BF16),
        pltpu.VMEM((2048, 256), BF16),
        pltpu.VMEM((256, 2048), BF16),
        pltpu.VMEM((NTP, TOK, W), BF16),
        pltpu.VMEM((64, 1024), F32),
        pltpu.VMEM((64, 1024), F32),
        pltpu.VMEM((64, 256), F32),
        pltpu.VMEM((NTP, TOK, W), BF16),
        pltpu.VMEM((NTP, TOK, W), BF16),
        pltpu.VMEM((512, 64), BF16),
        pltpu.VMEM((128, 512), BF16),
        pltpu.VMEM((512, 512), BF16),
        pltpu.VMEM((512, 512), BF16),
        pltpu.VMEM((TOK, W), BF16),
        pltpu.VMEM((NTP, TOK, W), BF16),
        pltpu.VMEM((NEP, 8, 128), BF16),
        pltpu.VMEM((NTP, NEP, 8, 128), BF16),
        pltpu.VMEM((128, 2048), BF16),
        pltpu.VMEM((NTP, TOK, W), BF16),
        pltpu.VMEM((NTP, TOK, W), BF16),
        pltpu.VMEM((NTP, 128, W), BF16),
        pltpu.VMEM((NTP, 128, W), BF16),
        pltpu.VMEM((NEP, 8, 128), BF16),
        pltpu.VMEM((NEP, 8, 128), BF16),
        pltpu.VMEM((16, 128), F32),
        dma((20,)),
        dma((4,)),
        dma,
        dma((NTP,)),
        regular,
        regular,
        dma,
        dma((NTP,)),
        dma,
        dma((NTP,)),
        dma,
        dma((NZ,)),
        dma,
        dma((NTP,)),
        dma,
        dma((NTP,)),
        dma,
        dma((NTP,)),
        dma,
        dma,
    ]
    return pl.pallas_call(
        layer,
        out_shape=pltpu.VMEM((TOK, W), BF16),
        in_specs=[hbm] * 21,
        out_specs=vmem,
        scratch_shapes=scratch,
        compiler_params=pltpu.CompilerParams(collective_id=0, has_side_effects=True),
        name="layer",
    )(
        tokens,
        lengths,
        forget_bias,
        attn_gain.reshape(16, 128),
        ffn_gain.reshape(16, 128),
        mix_gate.reshape(16, 128),
        chosen.T,
        route_weight.T,
        kv_cache,
        cum_gate,
        w_query,
        w_key.T,
        w_value.T,
        w_forget.T,
        w_out,
        expert_gate[0],
        expert_up[0],
        expert_down[0],
        dense_gate,
        dense_up,
        dense_down,
    )


def solution(mesh):
    in_specs = (
        P("ep", "tp"),
        P("ep", None, "tp"),
        P("ep", "tp", None),
        P("ep"),
        P(None, "tp"),
        P(None, "tp"),
        P(None, "tp"),
        P(None, "tp"),
        P("tp"),
        P("tp", None),
        P(),
        P(),
        P(),
        P("ep", None, "tp"),
        P("ep", None, "tp"),
        P("ep", "tp", None),
        P("ep", None),
        P("ep", None),
        P(None, "tp"),
        P(None, "tp"),
        P("tp", None),
    )
    out_specs = P("ep", "tp")
    return jax.shard_map(local, mesh=mesh, in_specs=in_specs, out_specs=out_specs, check_vma=False)
```

```python
import jax
import jax.numpy as jnp
from jax import lax
from jax.experimental import pallas as pl
from jax.experimental.pallas import tpu as pltpu
from jax.sharding import PartitionSpec as P

EPS = 1e-06
F32 = jnp.float32
BF16 = jnp.bfloat16
MESH = pl.DeviceIdType.MESH
ANY = pl.ANY

TOK = 16
HD = 64
NTP = 4
NZ = 8
NR = 8
NEP = 64
W = 512
NEAR = 3
SN = NEAR * NR
SF = NEP - SN
SB = 16
SA = SF - SB
ORDER = (0, 1, 7, 2, 6, 3, 5, 4)
NT = (((1,), (1,)), ((), ()))


def iota(shape, dim):
    return lax.broadcasted_iota(jnp.int32, shape, dim)


def dot(a, b):
    return jnp.dot(a, b, preferred_element_type=F32)


def dot_nt(a, b):
    return lax.dot_general(a, b, NT, preferred_element_type=F32)


def one_hot(mask):
    return jnp.where(mask, 1.0, 0.0).astype(BF16)


def three_parts(a):
    hi = a.astype(BF16)
    rest = a - hi.astype(F32)
    mid = rest.astype(BF16)
    low = (rest - mid.astype(F32)).astype(BF16)
    return hi, mid, low


def gain_row(gain_ref):
    gain = gain_ref[...].astype(F32)
    return jnp.concatenate([gain[j : j + 1, :] for j in range(16)], axis=1)


def silu(a):
    return a * (1.0 / (1.0 + jnp.exp(-a)))


def layer(
    tokens_hbm,
    lengths_hbm,
    bias_hbm,
    attn_hbm,
    ffn_hbm,
    mix_hbm,
    chosen_hbm,
    route_hbm,
    kv_hbm,
    cum_hbm,
    wq_hbm,
    wk_hbm,
    wv_hbm,
    wf_hbm,
    wo_hbm,
    eg_hbm,
    eu_hbm,
    ed_hbm,
    dg_hbm,
    du_hbm,
    dd_hbm,
    out,
    tokens,
    lengths,
    forget_bias,
    attn_gain,
    ffn_gain,
    mix_gate,
    chosen,
    route_weight,
    kv,
    keys,
    values,
    cum,
    wq,
    wkv,
    wf,
    wo,
    eg,
    eu,
    ed,
    dg,
    du,
    dd,
    xbuf,
    gate,
    sc,
    ob,
    pbuf,
    abuf,
    dmat,
    rmat_n,
    rmat_f,
    perm_n,
    permt_n,
    perm_b,
    permt_b,
    resb,
    rbuf,
    outg,
    outn,
    gath,
    hbuf,
    dpart,
    dsend,
    dbuf,
    ysend,
    ybuf,
    rout,
    routn,
    rin,
    rinn,
    ffn32,
    load_sem,
    kv_sem,
    x_send,
    x_recv,
    ready_a,
    ready_b,
    p_send,
    p_recv,
    r_send,
    r_recv,
    o_send,
    o_recv,
    g_send,
    g_recv,
    d_send,
    d_recv,
    y_send,
    y_recv,
    b_send,
    b_recv,
    n_send,
    c_send,
    c_recv,
):
    ep = lax.axis_index("ep")
    tp = lax.axis_index("tp")
    z = ep // NR
    r = lax.rem(ep, NR)
    peers = [lax.rem(tp + i, NTP) for i in (2, 1, 3)]
    planes = [lax.rem(z + i, NZ) for i in range(NZ)]
    mates = [lax.rem(r + i, NR) for i in range(NR)]

    def load(src, dst, i):
        copy = pltpu.make_async_copy(src, dst, load_sem.at[i])
        copy.start()
        return copy

    def remote(src, dst, send, recv, device):
        return pltpu.make_async_remote_copy(
            src_ref=src,
            dst_ref=dst,
            send_sem=send,
            recv_sem=recv,
            device_id=device,
            device_id_type=MESH,
        )

    def arrived(ref, sem):
        remote(ref, ref, x_send, sem, {"tp": peers[0]}).wait_recv()

    def left(ref, sem):
        remote(ref, ref, sem, x_recv.at[0], {"tp": peers[0]}).wait_send()

    loads = {}
    loads["tokens"] = load(tokens_hbm, tokens, 12)
    barrier = pltpu.get_barrier_semaphore()
    for p in peers:
        pl.semaphore_signal(barrier, inc=1, device_id={"tp": p}, device_id_type=MESH)
    for i in range(1, NR):
        pl.semaphore_signal(
            barrier, inc=1, device_id={"ep": z * NR + mates[i]}, device_id_type=MESH
        )
    for i in (1, 2, 6, 7):
        pl.semaphore_signal(
            barrier, inc=1, device_id={"ep": planes[i] * NR + r}, device_id_type=MESH
        )

    loads["lengths"] = load(lengths_hbm, lengths, 13)
    loads["cum"] = load(cum_hbm, cum, 0)
    loads["chosen"] = load(chosen_hbm, chosen, 14)
    loads["route"] = load(route_hbm, route_weight, 15)
    loads["attn"] = load(attn_hbm, attn_gain, 16)
    loads["ffn"] = load(ffn_hbm, ffn_gain, 17)
    loads["mix"] = load(mix_hbm, mix_gate, 18)
    loads["bias"] = load(bias_hbm, forget_bias, 19)

    def kv_load(q):
        part = pl.ds(4 * q, 4)
        return pltpu.make_async_copy(kv_hbm.at[part], kv.at[part], kv_sem.at[q])

    for q in range(4):
        kv_load(q).start()
    loads["wk"] = load(wk_hbm, wkv.at[pl.ds(0, 64)], 1)
    loads["wv"] = load(wv_hbm, wkv.at[pl.ds(64, 64)], 2)
    loads["wf"] = load(wf_hbm, wf, 3)
    loads["wq"] = load(wq_hbm, wq, 4)
    loads["tokens"].wait()
    pl.semaphore_wait(barrier, 14)

    for p in peers:
        remote(tokens, xbuf.at[tp], x_send, x_recv.at[tp], {"tp": p}).start()
    for i in (2, 6):
        pl.semaphore_signal(
            ready_a, inc=1, device_id={"ep": planes[i] * NR + r}, device_id_type=MESH
        )
    xbuf[tp] = tokens[...]
    loads["wo"] = load(wo_hbm, wo, 5)
    loads["dg"] = load(dg_hbm, dg, 6)
    loads["du"] = load(du_hbm, du, 7)
    loads["dd"] = load(dd_hbm, dd, 8)
    loads["eg"] = load(eg_hbm, eg, 9)
    loads["eu"] = load(eu_hbm, eu, 10)
    loads["ed"] = load(ed_hbm, ed, 11)

    for name in ("lengths", "cum"):
        loads[name].wait()

    def gate_pair(p, carry):
        both = jnp.concatenate([cum[2 * p], cum[2 * p + 1]], axis=0)
        row = iota((8, 1024), 0)
        pos = iota((8, 1024), 1)
        length = jnp.where(row < 4, lengths[2 * p], lengths[2 * p + 1])
        last = jnp.sum(jnp.where(pos == length - 1, both, 0.0), axis=1, keepdims=True)
        gate[pl.ds(pl.multiple_of(8 * p, 8), 8), :] = jnp.where(
            pos < length, last - both, -jnp.inf
        )
        return carry

    lax.fori_loop(0, 8, gate_pair, 0)

    def key_part(q, carry):
        kv_load(q).wait()
        for i in range(4):
            turned = jnp.transpose(kv[4 * q + i])
            keys[q, 64 * i : 64 * i + 64, :] = turned[0:64]
        for i in range(2):
            s = 4 * q + 2 * i
            values[q, :, 128 * i : 128 * i + 128] = jnp.concatenate(
                [kv[s][:, HD:128], kv[s + 1][:, HD:128]], axis=1
            )
        return carry

    lax.fori_loop(0, 4, key_part, 0)

    pl.semaphore_wait(ready_a, 2)
    for i in range(1, NR):
        pl.semaphore_signal(
            ready_b, inc=1, device_id={"ep": z * NR + mates[i]}, device_id_type=MESH
        )

    for name in ("attn", "bias"):
        loads[name].wait()
    for p in peers:
        arrived(xbuf.at[p], x_recv.at[p])
    x_full = jnp.concatenate([xbuf[p] for p in range(NTP)], axis=1).astype(F32)
    square = jnp.mean(x_full * x_full, axis=1, keepdims=True)
    h_one = (x_full * lax.rsqrt(square + EPS) * gain_row(attn_gain)).astype(BF16)

    for name in ("wk", "wv", "wf", "wq"):
        loads[name].wait()
    query = dot(h_one, wq[...]).astype(BF16)
    kv_new = dot_nt(h_one, wkv[...]).astype(BF16)
    forget = dot_nt(h_one, wf[...])
    head_lane = iota((TOK, 4), 1)
    bias = jnp.zeros((TOK, 4), F32)
    for h in range(4):
        bias = jnp.where(head_lane == h, forget_bias[h], bias)
    forget = forget + bias
    forget = jnp.minimum(forget, 0.0) - jnp.log1p(jnp.exp(-jnp.abs(forget)))

    row64 = iota((64, TOK), 0)
    col16 = iota((64, TOK), 1)
    repeat = one_hot(row64 // 4 == col16)
    row32 = iota((64, 32), 0)
    col32 = iota((64, 32), 1)
    even = one_hot((row32 // 4 == col32 % TOK) & (row32 % 4 == (col32 // TOK) * 2))
    odd = one_hot((row32 // 4 == col32 % TOK) & (row32 % 4 == (col32 // TOK) * 2 + 1))
    stacked = jnp.concatenate([query[:, 0:128], query[:, 128:256]], axis=0)
    low_half = iota((64, 128), 1) < HD
    q64 = jnp.where(
        low_half, dot(even, stacked) + pltpu.roll(dot(odd, stacked), HD, 1), 0.0
    )
    kv64 = dot(repeat, kv_new)
    f_parts = three_parts(forget)
    f64 = dot(repeat, f_parts[0]) + dot(repeat, f_parts[1]) + dot(repeat, f_parts[2])
    f64 = jnp.sum(
        jnp.where(iota((64, 4), 0) % 4 == iota((64, 4), 1), f64, 0.0), axis=1, keepdims=True
    )
    scale = HD ** (-0.5)
    own = jnp.sum(q64 * kv64, axis=1, keepdims=True) * scale - f64
    wide = jnp.concatenate([q64, q64], axis=1)
    wide = wide + pltpu.roll(wide, HD, 1)
    own_lanes = (iota((64, 256), 0) // 4) % 4 == iota((64, 256), 1) // HD
    blocks = jnp.where(own_lanes, wide, 0.0).astype(BF16)
    for q in range(4):
        sc[pl.ds(16 * q, 16), :] = dot(blocks[16 * q : 16 * q + 16], keys[q])
    score = sc[...] * scale + gate[...]
    highest = jnp.maximum(jnp.max(score, axis=1, keepdims=True), own)
    prob = jnp.exp(score - highest)
    own_prob = jnp.exp(own - highest)
    total = jnp.sum(prob, axis=1, keepdims=True) + own_prob
    inverse = 1.0 / total
    sc[...] = prob * inverse
    own_prob = own_prob * inverse
    for q in range(4):
        ob[pl.ds(16 * q, 16), :] = dot(sc[pl.ds(16 * q, 16), :].astype(BF16), values[q])
    seq = (iota((64, 128), 0) // 4) % 4
    blended = jnp.where(seq < 2, ob[:, 0:128], ob[:, 128:256])
    blended = jnp.where(seq % 2 == 0, pltpu.roll(blended, HD, 1), blended)
    blended = (blended + own_prob.astype(BF16).astype(F32) * kv64).astype(BF16)
    back = one_hot(
        iota((64, 64), 1) == (iota((64, 64), 0) % TOK) * 4 + iota((64, 64), 0) // TOK
    )
    heads = dot(back, blended)
    low16 = iota((TOK, 128), 1) < HD
    head_out = jnp.concatenate(
        [
            jnp.where(low16, pltpu.roll(heads[0:16], HD, 1), heads[16:32]),
            jnp.where(low16, pltpu.roll(heads[32:48], HD, 1), heads[48:64]),
        ],
        axis=1,
    ).astype(BF16)
    loads["wo"].wait()
    partial = dot(head_out, wo[...]).astype(BF16)
    for p in range(NTP):
        pbuf[p] = partial[:, p * W : (p + 1) * W]
    for p in peers:
        remote(pbuf.at[p], abuf.at[tp], p_send, p_recv.at[tp], {"tp": p}).start()
    abuf[tp] = pbuf[tp]

    for name in ("chosen", "route"):
        loads[name].wait()
    pick = chosen[...]
    expert = iota((NEP, TOK), 0)
    hot = [jnp.where(expert == pick[k : k + 1, :], 1.0, 0.0) for k in range(2)]
    earlier = one_hot(iota((TOK, TOK), 0) < iota((TOK, TOK), 1))
    before = dot((hot[0] + hot[1]).astype(BF16), earlier)
    away = lax.rem(pick // NR - z + NZ, NZ)
    order = jnp.where(away <= 4, jnp.maximum(2 * away - 1, 0), 16 - 2 * away)
    place = 2.0 * (order * NR + lax.rem(pick, NR)).astype(F32)
    slots = [
        place[k : k + 1, :] + jnp.sum(hot[k] * before, axis=0, keepdims=True)
        for k in range(2)
    ]
    weight = route_weight[...]
    w_rows = [three_parts(weight[k : k + 1, :]) for k in range(2)]
    info = jnp.concatenate(
        slots + [part.astype(F32) for k in range(2) for part in w_rows[k]], axis=0
    ).astype(BF16)
    spread = one_hot(iota((TOK, 64), 0) == iota((TOK, 64), 1) % TOK)
    spread_t = one_hot(iota((64, TOK), 0) % TOK == iota((64, TOK), 1))
    info_rows = dot(info, spread).astype(jnp.int32)
    info_cols = dot_nt(spread_t, info)
    row = iota((512, 64), 0)
    col_fb = iota((512, 64), 1) // TOK
    dmask = jnp.zeros((512, 64), F32)
    for k in range(2):
        dmask = dmask + jnp.where(row == info_rows[k : k + 1, :] * 4 + col_fb, 1.0, 0.0)
    dmat[...] = dmask.astype(BF16)
    for k in range(2):
        slot_col = info_cols[:, k : k + 1].astype(jnp.int32) * 4
        for ref, lo, n in ((rmat_n, 0, 8 * SN), (rmat_f, 8 * SN, 8 * SF)):
            lane = iota((64, n), 1) + lo
            row_fb = iota((64, n), 0) // TOK
            ref[pl.ds(64 * k, 64), :] = one_hot(lane == slot_col + row_fb)
    w_cols = [
        info_cols[:, 2 + 3 * k : 3 + 3 * k]
        + info_cols[:, 3 + 3 * k : 4 + 3 * k]
        + info_cols[:, 4 + 3 * k : 5 + 3 * k]
        for k in range(2)
    ]

    for n, ref, ref_t in ((SN, perm_n, permt_n), (SB, perm_b, permt_b)):

        def perm_part(i, carry, n=n, ref=ref, ref_t=ref_t):
            base = pl.multiple_of(64 * i, 64)
            a = iota((64, 8 * n), 0) + base
            b = iota((64, 8 * n), 1)
            ref[pl.ds(base, 64), :] = one_hot(lax.rem(a, 2 * n) * 4 + a // (2 * n) == b)
            ref_t[pl.ds(base, 64), :] = one_hot(lax.rem(b, 2 * n) * 4 + b // (2 * n) == a)
            return carry

        lax.fori_loop(0, n // 8, perm_part, 0)

    for name in ("ffn", "mix"):
        loads[name].wait()
    ffn32[...] = ffn_gain[...].astype(F32)
    pl.semaphore_wait(ready_b, 7)

    for p in peers:
        arrived(abuf.at[p], p_recv.at[p])
    attention = abuf[0].astype(F32)
    for p in range(1, NTP):
        attention = attention + abuf[p].astype(F32)
    residual = (tokens[...].astype(F32) + attention).astype(BF16)
    resb[...] = residual
    for p in peers:
        remote(resb, rbuf.at[tp], r_send, r_recv.at[tp], {"tp": p}).start()
    rbuf[tp] = residual

    def stack(rows):
        return jnp.concatenate([rows[:, f * 128 : (f + 1) * 128] for f in range(4)], axis=0)

    def unstack(rows):
        return jnp.concatenate([rows[16 * f : 16 * f + 16] for f in range(4)], axis=1)

    def block(b):
        return ORDER.index((NZ - ORDER[b]) % NZ)

    def mine(b):
        return block(b) * NR + r

    outgoing = dot(dmat[pl.ds(8 * SN, 8 * SF), :], stack(residual))
    outg[...] = outgoing.reshape(SF, 8, 128).astype(BF16)
    for b in range(NEAR, NZ):
        dz = ORDER[b]
        for i in range(1, NR + 1):
            m = mates[i % NR]
            remote(
                outg.at[(b - NEAR) * NR + m],
                gath.at[tp, mine(b)],
                o_send,
                o_recv.at[block(b)],
                {"ep": planes[dz] * NR + m},
            ).start()
    for p in peers:
        arrived(rbuf.at[p], r_recv.at[p])
    for q in range(NTP):
        outgoing = dot(dmat[pl.ds(0, 8 * SN), :], stack(rbuf[q]))
        outn[:, q] = outgoing.reshape(SN, 8, 128).astype(BF16)
    for b in range(NEAR):
        dz = ORDER[b]
        for i in range(1, NR + 1):
            if b or i < NR:
                m = mates[i % NR]
                remote(
                    outn.at[b * NR + m],
                    gath.at[:, mine(b)],
                    n_send,
                    o_recv.at[block(b)],
                    {"ep": planes[dz] * NR + m},
                ).start()
    gath[:, r] = outn[r]

    for b in range(NEAR, NZ):
        chunk = gath.at[tp, pl.ds(b * NR, NR)]
        arrived(chunk, o_recv.at[b])
        for p in peers:
            half = 0 if b < NEAR + 2 else 1
            remote(chunk, chunk, g_send, g_recv.at[half, tp], {"tp": p}).start()

    res_full = jnp.concatenate([rbuf[p] for p in range(NTP)], axis=1).astype(F32)
    square = jnp.mean(res_full * res_full, axis=1, keepdims=True)
    ffn_row = gain_row(ffn_gain)
    h_two = (res_full * lax.rsqrt(square + EPS) * ffn_row).astype(BF16)
    for name in ("dg", "du", "dd"):
        loads[name].wait()
    dense_act = (silu(dot(h_two, dg[...])) * dot(h_two, du[...])).astype(BF16)
    mixing = jnp.sum(h_two.astype(F32) * gain_row(mix_gate), axis=1, keepdims=True)
    blend = 1.0 / (1.0 + jnp.exp(-mixing))
    dpart[...] = dot(dense_act, dd[...]) * blend
    for name in ("eg", "eu", "ed"):
        loads[name].wait()

    def expert_hidden(lo, n, perm, sources):
        squares = jnp.zeros((2 * n, 128), F32)
        for p, sem in sources:
            if sem is not None:
                arrived(gath.at[p, pl.ds(lo, n)], sem)
            rows = dot(perm[...], gath[p, pl.ds(lo, n)].reshape(8 * n, 128))
            for f in range(4):
                part = rows[2 * n * f : 2 * n * (f + 1)]
                squares = squares + part * part
                c = p * 4 + f
                scaled = part * ffn32[pl.ds(c, 1), :]
                start = c * 128 if isinstance(c, int) else pl.multiple_of(c * 128, 128)
                hbuf[2 * lo : 2 * (lo + n), pl.ds(start, 128)] = scaled.astype(BF16)
        return lax.rsqrt(jnp.sum(squares, axis=1, keepdims=True) * (1.0 / 2048.0) + EPS)

    for b in range(NEAR):
        lo = 0 if b else 1
        arrived(gath.at[:, pl.ds(b * NR + lo, NR - lo)], o_recv.at[b])
    root_n = expert_hidden(0, SN, perm_n, [(p, None) for p in range(NTP)])
    others = [lax.rem(tp + i, NTP) for i in (1, 3, 2)]
    root_b = expert_hidden(
        SN, SB, perm_b, [(tp, None)] + [(p, g_recv.at[0, p]) for p in others]
    )
    root_a = expert_hidden(
        SN + SB, SA, perm_n, [(tp, None)] + [(p, g_recv.at[1, p]) for p in others]
    )
    root = jnp.concatenate([root_n, root_b, root_a], axis=0)
    hidden = hbuf[...]
    gate_pre = dot(hidden, eg[...]) * root
    up_pre = dot(hidden, eu[...]) * root
    act = (silu(gate_pre) * up_pre).astype(BF16)
    act_f = act[2 * SN : 128]
    for p in peers:
        ysend[p] = dot(act_f, ed[:, pl.ds(pl.multiple_of(p * W, W), W)]).astype(BF16)
        part = pl.ds(2 * SB, 2 * SA)
        remote(
            ysend.at[p, part], ybuf.at[tp, part], y_send, y_recv.at[1, tp], {"tp": p}
        ).start()
    for p in peers:
        part = pl.ds(0, 2 * SB)
        remote(
            ysend.at[p, part], ybuf.at[tp, part], y_send, y_recv.at[0, tp], {"tp": p}
        ).start()
    act_n = act[0 : 2 * SN]
    for q in range(NTP):
        part = dot(act_n, ed[:, q * W : (q + 1) * W]).astype(BF16)
        turned = dot(permt_n[...], stack(part))
        routn[:, q] = turned.reshape(SN, 8, 128).astype(BF16)
    for b in range(NEAR):
        dz = ORDER[b]
        for i in range(1, NR + 1):
            if b or i < NR:
                m = mates[i % NR]
                remote(
                    routn.at[b * NR + m],
                    rinn.at[mine(b)],
                    c_send,
                    c_recv,
                    {"ep": planes[dz] * NR + m},
                ).start()
    rinn[r] = routn[r]

    summed = dot(act_f, ed[:, pl.ds(pl.multiple_of(tp * W, W), W)]).astype(BF16).astype(F32)
    for half, lo, n, turn, first, last in (
        (1, SB, SA, permt_n, NEAR + 2, NZ),
        (0, 0, SB, permt_b, NEAR, NEAR + 2),
    ):
        rows = summed[2 * lo : 2 * (lo + n)]
        for p in peers:
            part = pl.ds(2 * lo, 2 * n)
            arrived(ybuf.at[p, part], y_recv.at[half, p])
            rows = rows + ybuf[p, part].astype(F32)
        turned = dot(turn[...], stack(rows.astype(BF16)))
        rout[pl.ds(lo, n)] = turned.reshape(n, 8, 128).astype(BF16)
        for b in reversed(range(first, last)):
            dz = ORDER[b]
            for i in range(1, NR + 1):
                m = mates[i % NR]
                remote(
                    rout.at[(b - NEAR) * NR + m],
                    rin.at[mine(b) - SN],
                    b_send,
                    b_recv,
                    {"ep": planes[dz] * NR + m},
                ).start()

    def routed(picked):
        return unstack(picked[0:64] * w_cols[0] + picked[64:128] * w_cols[1])

    arrived(rinn.at[pl.ds(0, SN - 1)], c_recv)
    for i in (2, 1, 3, 0):
        q = lax.rem(tp + i, NTP)
        part = routed(dot(rmat_n[...], rinn[:, q].reshape(8 * SN, 128)))
        part = part + dpart[:, pl.ds(pl.multiple_of(q * W, W), W)]
        if i:
            dsend[q] = part.astype(BF16)
            remote(dsend.at[q], dbuf.at[tp], d_send, d_recv.at[tp], {"tp": q}).start()
        else:
            mixed = residual.astype(F32) + part

    arrived(rin, b_recv)
    mixed = mixed + routed(dot(rmat_f[...], rin[...].reshape(8 * SF, 128)))
    for p in peers:
        arrived(dbuf.at[p], d_recv.at[p])
        mixed = mixed + dbuf[p].astype(F32)
    out[...] = mixed.astype(BF16)

    left(xbuf.at[pl.ds(0, 3)], x_send)
    left(pbuf.at[pl.ds(0, 3)], p_send)
    left(rbuf.at[pl.ds(0, 3)], r_send)
    left(outg, o_send)
    left(outn.at[pl.ds(0, SN - 1)], n_send)
    left(gath.at[pl.ds(0, 3), pl.ds(SN, SF)], g_send)
    left(dsend.at[pl.ds(0, 3)], d_send)
    left(ysend.at[pl.ds(0, 3)], y_send)
    left(rout, b_send)
    left(routn.at[pl.ds(0, SN - 1)], c_send)


def local(
    tokens,
    kv_cache,
    cum_gate,
    lengths,
    w_query,
    w_key,
    w_value,
    w_forget,
    forget_bias,
    w_out,
    attn_gain,
    ffn_gain,
    mix_gate,
    expert_gate,
    expert_up,
    expert_down,
    chosen,
    route_weight,
    dense_gate,
    dense_up,
    dense_down,
):
    vmem = pl.BlockSpec(memory_space=pltpu.VMEM)
    hbm = pl.BlockSpec(memory_space=ANY)
    dma = pltpu.SemaphoreType.DMA
    regular = pltpu.SemaphoreType.REGULAR
    scratch = [
        pltpu.VMEM((TOK, W), BF16),
        pltpu.SMEM((TOK,), jnp.int32),
        pltpu.SMEM((4,), F32),
        pltpu.VMEM((16, 128), BF16),
        pltpu.VMEM((16, 128), BF16),
        pltpu.VMEM((16, 128), BF16),
        pltpu.VMEM((2, TOK), jnp.int32),
        pltpu.VMEM((2, TOK), F32),
        pltpu.VMEM((TOK, 1024, 128), BF16),
        pltpu.VMEM((4, 256, 1024), BF16),
        pltpu.VMEM((4, 1024, 256), BF16),
        pltpu.VMEM((TOK, 4, 1024), F32),
        pltpu.VMEM((2048, 256), BF16),
        pltpu.VMEM((128, 2048), BF16),
        pltpu.VMEM((4, 2048), BF16),
        pltpu.VMEM((256, 2048), BF16),
        pltpu.VMEM((2048, 256), BF16),
        pltpu.VMEM((2048, 256), BF16),
        pltpu.VMEM((256, 2048), BF16),
        pltpu.VMEM((2048, 256), BF16),
        pltpu.VMEM((2048, 256), BF16),
        pltpu.VMEM((256, 2048), BF16),
        pltpu.VMEM((NTP, TOK, W), BF16),
        pltpu.VMEM((64, 1024), F32),
        pltpu.VMEM((64, 1024), F32),
        pltpu.VMEM((64, 256), F32),
        pltpu.VMEM((NTP, TOK, W), BF16),
        pltpu.VMEM((NTP, TOK, W), BF16),
        pltpu.VMEM((512, 64), BF16),
        pltpu.VMEM((128, 8 * SN), BF16),
        pltpu.VMEM((128, 8 * SF), BF16),
        pltpu.VMEM((8 * SN, 8 * SN), BF16),
        pltpu.VMEM((8 * SN, 8 * SN), BF16),
        pltpu.VMEM((8 * SB, 8 * SB), BF16),
        pltpu.VMEM((8 * SB, 8 * SB), BF16),
        pltpu.VMEM((TOK, W), BF16),
        pltpu.VMEM((NTP, TOK, W), BF16),
        pltpu.VMEM((SF, 8, 128), BF16),
        pltpu.VMEM((SN, NTP, 8, 128), BF16),
        pltpu.VMEM((NTP, NEP, 8, 128), BF16),
        pltpu.VMEM((128, 2048), BF16),
        pltpu.VMEM((TOK, 2048), F32),
        pltpu.VMEM((NTP, TOK, W), BF16),
        pltpu.VMEM((NTP, TOK, W), BF16),
        pltpu.VMEM((NTP, 2 * SF, W), BF16),
        pltpu.VMEM((NTP, 2 * SF, W), BF16),
        pltpu.VMEM((SF, 8, 128), BF16),
        pltpu.VMEM((SN, NTP, 8, 128), BF16),
        pltpu.VMEM((SF, 8, 128), BF16),
        pltpu.VMEM((SN, NTP, 8, 128), BF16),
        pltpu.VMEM((16, 128), F32),
        dma((20,)),
        dma((4,)),
        dma,
        dma((NTP,)),
        regular,
        regular,
        dma,
        dma((NTP,)),
        dma,
        dma((NTP,)),
        dma,
        dma((NZ,)),
        dma,
        dma((2, NTP)),
        dma,
        dma((NTP,)),
        dma,
        dma((2, NTP)),
        dma,
        dma,
        dma,
        dma,
        dma,
    ]
    return pl.pallas_call(
        layer,
        out_shape=pltpu.VMEM((TOK, W), BF16),
        in_specs=[hbm] * 21,
        out_specs=vmem,
        scratch_shapes=scratch,
        compiler_params=pltpu.CompilerParams(collective_id=0, has_side_effects=True),
        name="layer",
    )(
        tokens,
        lengths,
        forget_bias,
        attn_gain.reshape(16, 128),
        ffn_gain.reshape(16, 128),
        mix_gate.reshape(16, 128),
        chosen.T,
        route_weight.T,
        kv_cache,
        cum_gate,
        w_query,
        w_key.T,
        w_value.T,
        w_forget.T,
        w_out,
        expert_gate[0],
        expert_up[0],
        expert_down[0],
        dense_gate,
        dense_up,
        dense_down,
    )


def solution(mesh):
    in_specs = (
        P("ep", "tp"),
        P("ep", None, "tp"),
        P("ep", "tp", None),
        P("ep"),
        P(None, "tp"),
        P(None, "tp"),
        P(None, "tp"),
        P(None, "tp"),
        P("tp"),
        P("tp", None),
        P(),
        P(),
        P(),
        P("ep", None, "tp"),
        P("ep", None, "tp"),
        P("ep", "tp", None),
        P("ep", None),
        P("ep", None),
        P(None, "tp"),
        P(None, "tp"),
        P("tp", None),
    )
    out_specs = P("ep", "tp")
    return jax.shard_map(local, mesh=mesh, in_specs=in_specs, out_specs=out_specs, check_vma=False)
```

```python
import jax
import jax.numpy as jnp
from jax import lax
from jax.experimental import pallas as pl
from jax.experimental.pallas import tpu as pltpu
from jax.sharding import PartitionSpec as P

EPS = 1e-06
F32 = jnp.float32
BF16 = jnp.bfloat16
MESH = pl.DeviceIdType.MESH
ANY = pl.ANY

TOK = 16
HD = 64
NTP = 4
NZ = 8
NR = 8
NEP = 64
W = 512
NEAR = 3
DIRECT = 5
SD = DIRECT * NR
SN = NEAR * NR
SF = NEP - SN
SB = 16
SA = SF - SB
ORDER = (0, 1, 7, 2, 6, 3, 5, 4)
NT = (((1,), (1,)), ((), ()))


def iota(shape, dim):
    return lax.broadcasted_iota(jnp.int32, shape, dim)


def dot(a, b):
    return jnp.dot(a, b, preferred_element_type=F32)


def dot_nt(a, b):
    return lax.dot_general(a, b, NT, preferred_element_type=F32)


def one_hot(mask):
    return jnp.where(mask, 1.0, 0.0).astype(BF16)


def three_parts(a):
    hi = a.astype(BF16)
    rest = a - hi.astype(F32)
    mid = rest.astype(BF16)
    low = (rest - mid.astype(F32)).astype(BF16)
    return hi, mid, low


def gain_row(gain_ref):
    gain = gain_ref[...].astype(F32)
    return jnp.concatenate([gain[j : j + 1, :] for j in range(16)], axis=1)


def silu(a):
    return a * (1.0 / (1.0 + jnp.exp(-a)))


def layer(
    tokens_hbm,
    lengths_hbm,
    bias_hbm,
    attn_hbm,
    ffn_hbm,
    mix_hbm,
    chosen_hbm,
    route_hbm,
    kv_hbm,
    cum_hbm,
    wq_hbm,
    wk_hbm,
    wv_hbm,
    wf_hbm,
    wo_hbm,
    eg_hbm,
    eu_hbm,
    ed_hbm,
    dg_hbm,
    du_hbm,
    dd_hbm,
    out,
    tokens,
    lengths,
    forget_bias,
    attn_gain,
    ffn_gain,
    mix_gate,
    chosen,
    route_weight,
    kv,
    keys,
    values,
    cum,
    wq,
    wkv,
    wf,
    wo,
    eg,
    eu,
    ed,
    dg,
    du,
    dd,
    xbuf,
    gate,
    sc,
    ob,
    pbuf,
    abuf,
    dmat,
    rmat_n,
    rmat_f,
    perm_n,
    permt_n,
    perm_b,
    permt_b,
    permt_c,
    rbuf,
    outg,
    outn,
    gath,
    hbuf,
    dpart,
    dsend,
    dbuf,
    ysend,
    ybuf,
    rout,
    routn,
    rin,
    rinn,
    ffn32,
    attn32,
    load_sem,
    kv_sem,
    x_send,
    x_recv,
    ready_a,
    ready_b,
    p_send,
    p_recv,
    r_recv,
    o_send,
    o_recv,
    g_send,
    g_recv,
    d_send,
    d_recv,
    y_send,
    y_recv,
    b_send,
    b_recv,
    n_send,
    c_send,
    c_recv,
):
    ep = lax.axis_index("ep")
    tp = lax.axis_index("tp")
    z = ep // NR
    r = lax.rem(ep, NR)
    peers = [lax.rem(tp + i, NTP) for i in (2, 1, 3)]
    planes = [lax.rem(z + i, NZ) for i in range(NZ)]
    mates = [lax.rem(r + i, NR) for i in range(NR)]

    def load(src, dst, i):
        copy = pltpu.make_async_copy(src, dst, load_sem.at[i])
        copy.start()
        return copy

    def remote(src, dst, send, recv, device):
        return pltpu.make_async_remote_copy(
            src_ref=src,
            dst_ref=dst,
            send_sem=send,
            recv_sem=recv,
            device_id=device,
            device_id_type=MESH,
        )

    def arrived(ref, sem):
        remote(ref, ref, x_send, sem, {"tp": peers[0]}).wait_recv()

    def left(ref, sem):
        remote(ref, ref, sem, x_recv.at[0], {"tp": peers[0]}).wait_send()

    loads = {}
    loads["tokens"] = load(tokens_hbm, tokens, 12)
    barrier = pltpu.get_barrier_semaphore()
    for p in peers:
        pl.semaphore_signal(barrier, inc=1, device_id={"tp": p}, device_id_type=MESH)
    for i in range(1, NR):
        pl.semaphore_signal(
            barrier, inc=1, device_id={"ep": z * NR + mates[i]}, device_id_type=MESH
        )
    for i in (1, 2, 6, 7):
        pl.semaphore_signal(
            barrier, inc=1, device_id={"ep": planes[i] * NR + r}, device_id_type=MESH
        )

    loads["lengths"] = load(lengths_hbm, lengths, 13)
    loads["cum"] = load(cum_hbm, cum, 0)
    loads["chosen"] = load(chosen_hbm, chosen, 14)
    loads["route"] = load(route_hbm, route_weight, 15)
    loads["attn"] = load(attn_hbm, attn_gain, 16)
    loads["ffn"] = load(ffn_hbm, ffn_gain, 17)
    loads["mix"] = load(mix_hbm, mix_gate, 18)
    loads["bias"] = load(bias_hbm, forget_bias, 19)

    def kv_load(q):
        part = pl.ds(4 * q, 4)
        return pltpu.make_async_copy(kv_hbm.at[part], kv.at[part], kv_sem.at[q])

    for q in range(4):
        kv_load(q).start()
    loads["wk"] = load(wk_hbm, wkv.at[pl.ds(0, 64)], 1)
    loads["wv"] = load(wv_hbm, wkv.at[pl.ds(64, 64)], 2)
    loads["wf"] = load(wf_hbm, wf, 3)
    loads["wq"] = load(wq_hbm, wq, 4)
    loads["tokens"].wait()
    pl.semaphore_wait(barrier, 14)

    for p in peers:
        remote(tokens, xbuf.at[tp], x_send, x_recv.at[tp], {"tp": p}).start()
    for i in (2, 6):
        pl.semaphore_signal(
            ready_a, inc=1, device_id={"ep": planes[i] * NR + r}, device_id_type=MESH
        )
    xbuf[tp] = tokens[...]
    loads["wo"] = load(wo_hbm, wo, 5)
    loads["dg"] = load(dg_hbm, dg, 6)
    loads["du"] = load(du_hbm, du, 7)
    loads["dd"] = load(dd_hbm, dd, 8)
    loads["eg"] = load(eg_hbm, eg, 9)
    loads["eu"] = load(eu_hbm, eu, 10)
    loads["ed"] = load(ed_hbm, ed, 11)

    for name in ("lengths", "cum"):
        loads[name].wait()

    def gate_pair(p, carry):
        both = jnp.concatenate([cum[2 * p], cum[2 * p + 1]], axis=0)
        row = iota((8, 1024), 0)
        pos = iota((8, 1024), 1)
        length = jnp.where(row < 4, lengths[2 * p], lengths[2 * p + 1])
        last = jnp.sum(jnp.where(pos == length - 1, both, 0.0), axis=1, keepdims=True)
        gate[pl.ds(pl.multiple_of(8 * p, 8), 8), :] = jnp.where(
            pos < length, last - both, -jnp.inf
        )
        return carry

    lax.fori_loop(0, 8, gate_pair, 0)

    def key_part(q, carry):
        kv_load(q).wait()
        for i in range(4):
            turned = jnp.transpose(kv[4 * q + i])
            keys[q, 64 * i : 64 * i + 64, :] = turned[0:64]
        for i in range(2):
            s = 4 * q + 2 * i
            values[q, :, 128 * i : 128 * i + 128] = jnp.concatenate(
                [kv[s][:, HD:128], kv[s + 1][:, HD:128]], axis=1
            )
        return carry

    lax.fori_loop(0, 4, key_part, 0)

    pl.semaphore_wait(ready_a, 2)
    for i in range(1, NR):
        pl.semaphore_signal(
            ready_b, inc=1, device_id={"ep": z * NR + mates[i]}, device_id_type=MESH
        )

    for name in ("attn", "bias"):
        loads[name].wait()
    attn32[...] = attn_gain[...].astype(F32)
    for name in ("wk", "wv", "wf", "wq"):
        loads[name].wait()
    squares = jnp.zeros((TOK, 128), F32)
    query = jnp.zeros((TOK, 256), F32)
    kv_new = jnp.zeros((TOK, 128), F32)
    forget = jnp.zeros((TOK, 4), F32)
    for i in (0, 1, 3, 2):
        p = lax.rem(tp + i, NTP)
        if i:
            arrived(xbuf.at[p], x_recv.at[p])
        rows = xbuf[p].astype(F32)
        scaled = []
        for f in range(4):
            part = rows[:, 128 * f : 128 * f + 128]
            squares = squares + part * part
            scaled.append((part * attn32[pl.ds(4 * p + f, 1), :]).astype(BF16))
        scaled = jnp.concatenate(scaled, axis=1)
        span = pl.ds(pl.multiple_of(p * W, W), W)
        query = query + dot(scaled, wq[span, :])
        kv_new = kv_new + dot_nt(scaled, wkv[:, span])
        forget = forget + dot_nt(scaled, wf[:, span])
    root = lax.rsqrt(jnp.sum(squares, axis=1, keepdims=True) * (1.0 / 2048.0) + EPS)
    query = (query * root).astype(BF16)
    kv_new = (kv_new * root).astype(BF16)
    forget = forget * root
    head_lane = iota((TOK, 4), 1)
    bias = jnp.zeros((TOK, 4), F32)
    for h in range(4):
        bias = jnp.where(head_lane == h, forget_bias[h], bias)
    forget = forget + bias
    forget = jnp.minimum(forget, 0.0) - jnp.log1p(jnp.exp(-jnp.abs(forget)))

    row64 = iota((64, TOK), 0)
    col16 = iota((64, TOK), 1)
    repeat = one_hot(row64 // 4 == col16)
    row32 = iota((64, 32), 0)
    col32 = iota((64, 32), 1)
    even = one_hot((row32 // 4 == col32 % TOK) & (row32 % 4 == (col32 // TOK) * 2))
    odd = one_hot((row32 // 4 == col32 % TOK) & (row32 % 4 == (col32 // TOK) * 2 + 1))
    stacked = jnp.concatenate([query[:, 0:128], query[:, 128:256]], axis=0)
    low_half = iota((64, 128), 1) < HD
    q64 = jnp.where(
        low_half, dot(even, stacked) + pltpu.roll(dot(odd, stacked), HD, 1), 0.0
    )
    kv64 = dot(repeat, kv_new)
    f_parts = three_parts(forget)
    f64 = dot(repeat, f_parts[0]) + dot(repeat, f_parts[1]) + dot(repeat, f_parts[2])
    f64 = jnp.sum(
        jnp.where(iota((64, 4), 0) % 4 == iota((64, 4), 1), f64, 0.0), axis=1, keepdims=True
    )
    scale = HD ** (-0.5)
    own = jnp.sum(q64 * kv64, axis=1, keepdims=True) * scale - f64
    wide = jnp.concatenate([q64, q64], axis=1)
    wide = wide + pltpu.roll(wide, HD, 1)
    own_lanes = (iota((64, 256), 0) // 4) % 4 == iota((64, 256), 1) // HD
    blocks = jnp.where(own_lanes, wide, 0.0).astype(BF16)
    for q in range(4):
        sc[pl.ds(16 * q, 16), :] = dot(blocks[16 * q : 16 * q + 16], keys[q])
    score = sc[...] * scale + gate[...]
    highest = jnp.maximum(jnp.max(score, axis=1, keepdims=True), own)
    prob = jnp.exp(score - highest)
    own_prob = jnp.exp(own - highest)
    total = jnp.sum(prob, axis=1, keepdims=True) + own_prob
    inverse = 1.0 / total
    sc[...] = prob
    for q in range(4):
        ob[pl.ds(16 * q, 16), :] = dot(sc[pl.ds(16 * q, 16), :].astype(BF16), values[q])
    seq = (iota((64, 128), 0) // 4) % 4
    blended = jnp.where(seq < 2, ob[:, 0:128], ob[:, 128:256])
    blended = jnp.where(seq % 2 == 0, pltpu.roll(blended, HD, 1), blended)
    blended = ((blended + own_prob * kv64) * inverse).astype(BF16)
    back = one_hot(
        iota((64, 64), 1) == (iota((64, 64), 0) % TOK) * 4 + iota((64, 64), 0) // TOK
    )
    heads = dot(back, blended)
    low16 = iota((TOK, 128), 1) < HD
    head_out = jnp.concatenate(
        [
            jnp.where(low16, pltpu.roll(heads[0:16], HD, 1), heads[16:32]),
            jnp.where(low16, pltpu.roll(heads[32:48], HD, 1), heads[48:64]),
        ],
        axis=1,
    ).astype(BF16)
    loads["wo"].wait()
    for p in peers:
        pbuf[p] = dot(head_out, wo[:, pl.ds(pl.multiple_of(p * W, W), W)]).astype(BF16)
        remote(pbuf.at[p], abuf.at[tp, p], p_send, p_recv.at[tp], {"tp": p}).start()
    pbuf[tp] = dot(head_out, wo[:, pl.ds(pl.multiple_of(tp * W, W), W)]).astype(BF16)
    for i in (1, 2, 3):
        for p in peers:
            q = lax.rem(p + i, NTP)
            remote(pbuf.at[q], abuf.at[tp, q], p_send, r_recv.at[tp], {"tp": p}).start()
    abuf[tp] = pbuf[...]

    for name in ("chosen", "route"):
        loads[name].wait()
    pick = chosen[...]
    expert = iota((NEP, TOK), 0)
    hot = [jnp.where(expert == pick[k : k + 1, :], 1.0, 0.0) for k in range(2)]
    earlier = one_hot(iota((TOK, TOK), 0) < iota((TOK, TOK), 1))
    before = dot((hot[0] + hot[1]).astype(BF16), earlier)
    away = lax.rem(pick // NR - z + NZ, NZ)
    order = jnp.where(away <= 4, jnp.maximum(2 * away - 1, 0), 16 - 2 * away)
    place = 2.0 * (order * NR + lax.rem(pick, NR)).astype(F32)
    slots = [
        place[k : k + 1, :] + jnp.sum(hot[k] * before, axis=0, keepdims=True)
        for k in range(2)
    ]
    weight = route_weight[...]
    w_rows = [three_parts(weight[k : k + 1, :]) for k in range(2)]
    info = jnp.concatenate(
        slots + [part.astype(F32) for k in range(2) for part in w_rows[k]], axis=0
    ).astype(BF16)
    spread = one_hot(iota((TOK, 64), 0) == iota((TOK, 64), 1) % TOK)
    spread_t = one_hot(iota((64, TOK), 0) % TOK == iota((64, TOK), 1))
    info_rows = dot(info, spread).astype(jnp.int32)
    info_cols = dot_nt(spread_t, info)
    row = iota((512, 64), 0)
    col_fb = iota((512, 64), 1) // TOK
    dmask = jnp.zeros((512, 64), F32)
    for k in range(2):
        dmask = dmask + jnp.where(row == info_rows[k : k + 1, :] * 4 + col_fb, 1.0, 0.0)
    dmat[...] = dmask.astype(BF16)
    for k in range(2):
        slot_col = info_cols[:, k : k + 1].astype(jnp.int32) * 4
        for ref, lo, n in ((rmat_n, 0, 8 * SN), (rmat_f, 8 * SN, 8 * SF)):
            lane = iota((64, n), 1) + lo
            row_fb = iota((64, n), 0) // TOK
            ref[pl.ds(64 * k, 64), :] = one_hot(lane == slot_col + row_fb)
    w_cols = [
        info_cols[:, 2 + 3 * k : 3 + 3 * k]
        + info_cols[:, 3 + 3 * k : 4 + 3 * k]
        + info_cols[:, 4 + 3 * k : 5 + 3 * k]
        for k in range(2)
    ]

    for n, ref, ref_t in ((SN, perm_n, permt_n), (SB, perm_b, permt_b), (NR, None, permt_c)):

        def perm_part(i, carry, n=n, ref=ref, ref_t=ref_t):
            base = 0 if n == NR else pl.multiple_of(64 * i, 64)
            a = iota((64, 8 * n), 0) + base
            b = iota((64, 8 * n), 1)
            if ref is not None:
                ref[pl.ds(base, 64), :] = one_hot(lax.rem(a, 2 * n) * 4 + a // (2 * n) == b)
            ref_t[pl.ds(base, 64), :] = one_hot(lax.rem(b, 2 * n) * 4 + b // (2 * n) == a)
            return carry

        if n > NR:
            lax.fori_loop(0, n // NR, perm_part, 0)
        else:
            perm_part(0, 0)

    for name in ("ffn", "mix"):
        loads[name].wait()
    ffn32[...] = ffn_gain[...].astype(F32)
    pl.semaphore_wait(ready_b, 7)

    for p in peers:
        arrived(abuf.at[p, tp], p_recv.at[p])
    def residual_of(q):
        attention = abuf[0, q].astype(F32)
        for p in range(1, NTP):
            attention = attention + abuf[p, q].astype(F32)
        return (xbuf[q].astype(F32) + attention).astype(BF16)

    residual = residual_of(tp)

    def stack(rows):
        return jnp.concatenate([rows[:, f * 128 : (f + 1) * 128] for f in range(4)], axis=0)

    def unstack(rows):
        return jnp.concatenate([rows[16 * f : 16 * f + 16] for f in range(4)], axis=1)

    def block(b):
        return ORDER.index((NZ - ORDER[b]) % NZ)

    def mine(b):
        return block(b) * NR + r

    outgoing = dot(dmat[pl.ds(8 * SD, 8 * SA), :], stack(residual))
    outg[...] = outgoing.reshape(SA, 8, 128).astype(BF16)
    for b in range(DIRECT, NZ):
        dz = ORDER[b]
        for i in range(1, NR + 1):
            m = mates[i % NR]
            remote(
                outg.at[(b - DIRECT) * NR + m],
                gath.at[tp, mine(b)],
                o_send,
                o_recv.at[block(b)],
                {"ep": planes[dz] * NR + m},
            ).start()
    for p in peers:
        arrived(abuf.at[p, pl.ds(0, 3)], r_recv.at[p])
    for q in range(NTP):
        rbuf[q] = residual_of(q)
    wide = jnp.concatenate([stack(rbuf[q]) for q in range(NTP)], axis=1)
    outgoing = dot(dmat[pl.ds(0, 8 * SD), :], wide)
    for q in range(NTP):
        outn[:, q] = outgoing[:, 128 * q : 128 * q + 128].reshape(SD, 8, 128).astype(BF16)
    for b in range(DIRECT):
        dz = ORDER[b]
        for i in range(1, NR + 1):
            if b or i < NR:
                m = mates[i % NR]
                remote(
                    outn.at[b * NR + m],
                    gath.at[:, mine(b)],
                    n_send,
                    o_recv.at[block(b)],
                    {"ep": planes[dz] * NR + m},
                ).start()
    gath[:, r] = outn[r]

    for b in range(DIRECT, NZ):
        chunk = gath.at[tp, pl.ds(b * NR, NR)]
        arrived(chunk, o_recv.at[b])
        for p in peers:
            remote(chunk, chunk, g_send, g_recv.at[tp], {"tp": p}).start()

    res_full = jnp.concatenate([rbuf[p] for p in range(NTP)], axis=1).astype(F32)
    square = jnp.mean(res_full * res_full, axis=1, keepdims=True)
    ffn_row = gain_row(ffn_gain)
    h_two = (res_full * lax.rsqrt(square + EPS) * ffn_row).astype(BF16)
    for name in ("dg", "du", "dd"):
        loads[name].wait()
    dense_act = (silu(dot(h_two, dg[...])) * dot(h_two, du[...])).astype(BF16)
    mixing = jnp.sum(h_two.astype(F32) * gain_row(mix_gate), axis=1, keepdims=True)
    blend = 1.0 / (1.0 + jnp.exp(-mixing))
    dpart[...] = dot(dense_act, dd[...]) * blend
    for name in ("eg", "eu", "ed"):
        loads[name].wait()

    def scaled_rows(rows, lo, n, c):
        start = c * 128 if isinstance(c, int) else pl.multiple_of(c * 128, 128)
        hbuf[2 * lo : 2 * (lo + n), pl.ds(start, 128)] = (rows * ffn32[pl.ds(c, 1), :]).astype(
            BF16
        )
        return rows * rows

    def root_of(squares):
        return lax.rsqrt(jnp.sum(squares, axis=1, keepdims=True) * (1.0 / 2048.0) + EPS)

    def direct_rows(lo, n, perm):
        wide = jnp.concatenate(
            [gath[q, pl.ds(lo, n)].reshape(8 * n, 128) for q in range(NTP)], axis=1
        )
        rows = dot(perm[...], wide)
        squares = jnp.zeros((2 * n, 128), F32)
        for q in range(NTP):
            for f in range(4):
                part = rows[2 * n * f : 2 * n * (f + 1), 128 * q : 128 * q + 128]
                squares = squares + scaled_rows(part, lo, n, 4 * q + f)
        return root_of(squares)

    for b in range(DIRECT):
        lo = 0 if b else 1
        arrived(gath.at[:, pl.ds(b * NR + lo, NR - lo)], o_recv.at[b])
    root_n = direct_rows(0, SN, perm_n)
    root_b = direct_rows(SN, SB, perm_b)
    root = jnp.concatenate([root_n, root_b], axis=0)
    hidden = hbuf[0 : 2 * SD]
    act_d = silu(dot(hidden, eg[...]) * root) * (dot(hidden, eu[...]) * root)
    act_d = act_d.astype(BF16)
    act_b = act_d[2 * SN : 2 * SD]
    part = pl.ds(0, 2 * SB)
    for p in peers:
        ysend[p, part] = dot(act_b, ed[:, pl.ds(pl.multiple_of(p * W, W), W)]).astype(BF16)
        remote(
            ysend.at[p, part], ybuf.at[tp, part], y_send, y_recv.at[0, tp], {"tp": p}
        ).start()
    squares = jnp.zeros((2 * SA, 128), F32)
    gate_pre = jnp.zeros((2 * SA, 256), F32)
    up_pre = jnp.zeros((2 * SA, 256), F32)
    for i in (0, 1, 3, 2):
        p = lax.rem(tp + i, NTP)
        if i:
            arrived(gath.at[p, pl.ds(SD, SA)], g_recv.at[p])
        rows = dot(perm_n[...], gath[p, pl.ds(SD, SA)].reshape(8 * SA, 128))
        for f in range(4):
            part = rows[2 * SA * f : 2 * SA * (f + 1)]
            squares = squares + scaled_rows(part, SD, SA, 4 * p + f)
        span = pl.ds(pl.multiple_of(p * W, W), W)
        hidden = hbuf[2 * SD : 128, span]
        gate_pre = gate_pre + dot(hidden, eg[span, :])
        up_pre = up_pre + dot(hidden, eu[span, :])
    root_a = root_of(squares)
    act_f = (silu(gate_pre * root_a) * (up_pre * root_a)).astype(BF16)
    for half, lo, n in ((2, 32, NR), (1, 16, SB)):
        part = pl.ds(2 * lo, 2 * n)
        for p in peers:
            if half == 2:
                ysend[p, pl.ds(2 * SB, 2 * SA)] = dot(
                    act_f, ed[:, pl.ds(pl.multiple_of(p * W, W), W)]
                ).astype(BF16)
            remote(
                ysend.at[p, part], ybuf.at[tp, part], y_send, y_recv.at[half, tp], {"tp": p}
            ).start()
    act_n = act_d[0 : 2 * SN]
    part = dot(act_n, ed[...]).astype(BF16)
    wide = jnp.concatenate([stack(part[:, q * W : (q + 1) * W]) for q in range(NTP)], axis=1)
    turned = dot(permt_n[...], wide)
    for q in range(NTP):
        routn[:, q] = turned[:, 128 * q : 128 * q + 128].reshape(SN, 8, 128).astype(BF16)
    for b in range(NEAR):
        dz = ORDER[b]
        for i in range(1, NR + 1):
            if b or i < NR:
                m = mates[i % NR]
                remote(
                    routn.at[b * NR + m],
                    rinn.at[mine(b)],
                    c_send,
                    c_recv,
                    {"ep": planes[dz] * NR + m},
                ).start()
    rinn[r] = routn[r]

    own_cols = ed[:, pl.ds(pl.multiple_of(tp * W, W), W)]
    sum_b = dot(act_b, own_cols).astype(BF16).astype(F32)
    sum_a = dot(act_f, own_cols).astype(BF16).astype(F32)
    for half, lo, n, turn, first, last, rows in (
        (0, 0, SB, permt_b, 3, 5, sum_b),
        (2, 32, NR, permt_c, 7, 8, sum_a[32:48]),
        (1, 16, SB, permt_b, 5, 7, sum_a[0:32]),
    ):
        for p in peers:
            part = pl.ds(2 * lo, 2 * n)
            arrived(ybuf.at[p, part], y_recv.at[half, p])
            rows = rows + ybuf[p, part].astype(F32)
        turned = dot(turn[...], stack(rows.astype(BF16)))
        rout[pl.ds(lo, n)] = turned.reshape(n, 8, 128).astype(BF16)
        for b in reversed(range(first, last)):
            dz = ORDER[b]
            for i in range(1, NR + 1):
                m = mates[i % NR]
                remote(
                    rout.at[(b - NEAR) * NR + m],
                    rin.at[mine(b) - SN],
                    b_send,
                    b_recv,
                    {"ep": planes[dz] * NR + m},
                ).start()

    def routed(picked):
        return unstack(picked[0:64] * w_cols[0] + picked[64:128] * w_cols[1])

    arrived(rinn.at[pl.ds(0, SN - 1)], c_recv)
    wide = jnp.concatenate([rinn[:, q].reshape(8 * SN, 128) for q in range(NTP)], axis=1)
    picked = dot(rmat_n[...], wide)
    for q in range(NTP):
        part = routed(picked[:, 128 * q : 128 * q + 128])
        dpart[:, q * W : (q + 1) * W] = part + dpart[:, q * W : (q + 1) * W]
    for i in (2, 1, 3, 0):
        q = lax.rem(tp + i, NTP)
        part = dpart[:, pl.ds(pl.multiple_of(q * W, W), W)]
        if i:
            dsend[q] = part.astype(BF16)
            remote(dsend.at[q], dbuf.at[tp], d_send, d_recv.at[tp], {"tp": q}).start()
        else:
            mixed = residual.astype(F32) + part

    arrived(rin, b_recv)
    mixed = mixed + routed(dot(rmat_f[...], rin[...].reshape(8 * SF, 128)))
    for p in peers:
        arrived(dbuf.at[p], d_recv.at[p])
        mixed = mixed + dbuf[p].astype(F32)
    out[...] = mixed.astype(BF16)

    left(xbuf.at[pl.ds(0, 3)], x_send)
    left(abuf.at[pl.ds(0, 3)], p_send)
    left(outg, o_send)
    left(outn.at[pl.ds(0, SD - 1)], n_send)
    left(gath.at[pl.ds(0, 3), pl.ds(SD, SA)], g_send)
    left(dsend.at[pl.ds(0, 3)], d_send)
    left(ysend.at[pl.ds(0, 3)], y_send)
    left(rout, b_send)
    left(routn.at[pl.ds(0, SN - 1)], c_send)


def local(
    tokens,
    kv_cache,
    cum_gate,
    lengths,
    w_query,
    w_key,
    w_value,
    w_forget,
    forget_bias,
    w_out,
    attn_gain,
    ffn_gain,
    mix_gate,
    expert_gate,
    expert_up,
    expert_down,
    chosen,
    route_weight,
    dense_gate,
    dense_up,
    dense_down,
):
    vmem = pl.BlockSpec(memory_space=pltpu.VMEM)
    hbm = pl.BlockSpec(memory_space=ANY)
    dma = pltpu.SemaphoreType.DMA
    regular = pltpu.SemaphoreType.REGULAR
    scratch = [
        pltpu.VMEM((TOK, W), BF16),
        pltpu.SMEM((TOK,), jnp.int32),
        pltpu.SMEM((4,), F32),
        pltpu.VMEM((16, 128), BF16),
        pltpu.VMEM((16, 128), BF16),
        pltpu.VMEM((16, 128), BF16),
        pltpu.VMEM((2, TOK), jnp.int32),
        pltpu.VMEM((2, TOK), F32),
        pltpu.VMEM((TOK, 1024, 128), BF16),
        pltpu.VMEM((4, 256, 1024), BF16),
        pltpu.VMEM((4, 1024, 256), BF16),
        pltpu.VMEM((TOK, 4, 1024), F32),
        pltpu.VMEM((2048, 256), BF16),
        pltpu.VMEM((128, 2048), BF16),
        pltpu.VMEM((4, 2048), BF16),
        pltpu.VMEM((256, 2048), BF16),
        pltpu.VMEM((2048, 256), BF16),
        pltpu.VMEM((2048, 256), BF16),
        pltpu.VMEM((256, 2048), BF16),
        pltpu.VMEM((2048, 256), BF16),
        pltpu.VMEM((2048, 256), BF16),
        pltpu.VMEM((256, 2048), BF16),
        pltpu.VMEM((NTP, TOK, W), BF16),
        pltpu.VMEM((64, 1024), F32),
        pltpu.VMEM((64, 1024), F32),
        pltpu.VMEM((64, 256), F32),
        pltpu.VMEM((NTP, TOK, W), BF16),
        pltpu.VMEM((NTP, NTP, TOK, W), BF16),
        pltpu.VMEM((512, 64), BF16),
        pltpu.VMEM((128, 8 * SN), BF16),
        pltpu.VMEM((128, 8 * SF), BF16),
        pltpu.VMEM((8 * SN, 8 * SN), BF16),
        pltpu.VMEM((8 * SN, 8 * SN), BF16),
        pltpu.VMEM((8 * SB, 8 * SB), BF16),
        pltpu.VMEM((8 * SB, 8 * SB), BF16),
        pltpu.VMEM((64, 64), BF16),
        pltpu.VMEM((NTP, TOK, W), BF16),
        pltpu.VMEM((SA, 8, 128), BF16),
        pltpu.VMEM((SD, NTP, 8, 128), BF16),
        pltpu.VMEM((NTP, NEP, 8, 128), BF16),
        pltpu.VMEM((128, 2048), BF16),
        pltpu.VMEM((TOK, 2048), F32),
        pltpu.VMEM((NTP, TOK, W), BF16),
        pltpu.VMEM((NTP, TOK, W), BF16),
        pltpu.VMEM((NTP, 2 * SF, W), BF16),
        pltpu.VMEM((NTP, 2 * SF, W), BF16),
        pltpu.VMEM((SF, 8, 128), BF16),
        pltpu.VMEM((SN, NTP, 8, 128), BF16),
        pltpu.VMEM((SF, 8, 128), BF16),
        pltpu.VMEM((SN, NTP, 8, 128), BF16),
        pltpu.VMEM((16, 128), F32),
        pltpu.VMEM((16, 128), F32),
        dma((20,)),
        dma((4,)),
        dma,
        dma((NTP,)),
        regular,
        regular,
        dma,
        dma((NTP,)),
        dma((NTP,)),
        dma,
        dma((NZ,)),
        dma,
        dma((NTP,)),
        dma,
        dma((NTP,)),
        dma,
        dma((3, NTP)),
        dma,
        dma,
        dma,
        dma,
        dma,
    ]
    return pl.pallas_call(
        layer,
        out_shape=pltpu.VMEM((TOK, W), BF16),
        in_specs=[hbm] * 21,
        out_specs=vmem,
        scratch_shapes=scratch,
        compiler_params=pltpu.CompilerParams(collective_id=0, has_side_effects=True),
        name="layer",
    )(
        tokens,
        lengths,
        forget_bias,
        attn_gain.reshape(16, 128),
        ffn_gain.reshape(16, 128),
        mix_gate.reshape(16, 128),
        chosen.T,
        route_weight.T,
        kv_cache,
        cum_gate,
        w_query,
        w_key.T,
        w_value.T,
        w_forget.T,
        w_out,
        expert_gate[0],
        expert_up[0],
        expert_down[0],
        dense_gate,
        dense_up,
        dense_down,
    )


def solution(mesh):
    in_specs = (
        P("ep", "tp"),
        P("ep", None, "tp"),
        P("ep", "tp", None),
        P("ep"),
        P(None, "tp"),
        P(None, "tp"),
        P(None, "tp"),
        P(None, "tp"),
        P("tp"),
        P("tp", None),
        P(),
        P(),
        P(),
        P("ep", None, "tp"),
        P("ep", None, "tp"),
        P("ep", "tp", None),
        P("ep", None),
        P("ep", None),
        P(None, "tp"),
        P(None, "tp"),
        P("tp", None),
    )
    out_specs = P("ep", "tp")
    return jax.shard_map(local, mesh=mesh, in_specs=in_specs, out_specs=out_specs, check_vma=False)
```

```python
import jax
import jax.numpy as jnp
from jax import lax
from jax.experimental import pallas as pl
from jax.experimental.pallas import tpu as pltpu
from jax.sharding import PartitionSpec as P

EPS = 1e-06
F32 = jnp.float32
BF16 = jnp.bfloat16
MESH = pl.DeviceIdType.MESH
ANY = pl.ANY

TOK = 16
HD = 64
NTP = 4
NZ = 8
NR = 8
NEP = 64
W = 512
NEAR = 3
DIRECT = 5
SD = DIRECT * NR
SN = NEAR * NR
SF = NEP - SN
SB = 16
SA = SF - SB
ORDER = (0, 1, 7, 2, 6, 3, 5, 4)
NT = (((1,), (1,)), ((), ()))


def iota(shape, dim):
    return lax.broadcasted_iota(jnp.int32, shape, dim)


def dot(a, b):
    return jnp.dot(a, b, preferred_element_type=F32)


def dot_nt(a, b):
    return lax.dot_general(a, b, NT, preferred_element_type=F32)


def one_hot(mask):
    return jnp.where(mask, 1.0, 0.0).astype(BF16)


def three_parts(a):
    hi = a.astype(BF16)
    rest = a - hi.astype(F32)
    mid = rest.astype(BF16)
    low = (rest - mid.astype(F32)).astype(BF16)
    return hi, mid, low


def gain_row(gain_ref):
    gain = gain_ref[...].astype(F32)
    return jnp.concatenate([gain[j : j + 1, :] for j in range(16)], axis=1)


def silu(a):
    return a * (1.0 / (1.0 + jnp.exp(-a)))


def layer(
    tokens_hbm,
    lengths_hbm,
    bias_hbm,
    attn_hbm,
    ffn_hbm,
    mix_hbm,
    chosen_hbm,
    route_hbm,
    kv_hbm,
    cum_hbm,
    wq_hbm,
    wk_hbm,
    wv_hbm,
    wf_hbm,
    wo_hbm,
    eg_hbm,
    eu_hbm,
    ed_hbm,
    dg_hbm,
    du_hbm,
    dd_hbm,
    out,
    tokens,
    lengths,
    forget_bias,
    attn_gain,
    ffn_gain,
    mix_gate,
    chosen,
    route_weight,
    kv,
    keys,
    values,
    cum,
    wq,
    wkv,
    wf,
    wo,
    eg,
    eu,
    ed,
    dg,
    du,
    dd,
    xbuf,
    gate,
    pbuf,
    abuf,
    dmat,
    rmat_n,
    rmat_f,
    perm_n,
    permt_n,
    perm_b,
    permt_b,
    permt_c,
    rbuf,
    outg,
    outn,
    gath,
    hbuf,
    dpart,
    dsend,
    dbuf,
    ysend,
    ybuf,
    rout,
    routn,
    rin,
    rinn,
    ffn32,
    attn32,
    load_sem,
    kv_sem,
    x_send,
    x_recv,
    ready_a,
    ready_b,
    p_send,
    p_recv,
    r_recv,
    o_send,
    o_recv,
    g_send,
    g_recv,
    d_send,
    d_recv,
    y_send,
    y_recv,
    b_send,
    b_recv,
    n_send,
    c_send,
    c_recv,
):
    ep = lax.axis_index("ep")
    tp = lax.axis_index("tp")
    z = ep // NR
    r = lax.rem(ep, NR)
    peers = [lax.rem(tp + i, NTP) for i in (2, 1, 3)]
    planes = [lax.rem(z + i, NZ) for i in range(NZ)]
    mates = [lax.rem(r + i, NR) for i in range(NR)]

    def load(src, dst, i):
        copy = pltpu.make_async_copy(src, dst, load_sem.at[i])
        copy.start()
        return copy

    def remote(src, dst, send, recv, device):
        return pltpu.make_async_remote_copy(
            src_ref=src,
            dst_ref=dst,
            send_sem=send,
            recv_sem=recv,
            device_id=device,
            device_id_type=MESH,
        )

    def arrived(ref, sem):
        remote(ref, ref, x_send, sem, {"tp": peers[0]}).wait_recv()

    def left(ref, sem):
        remote(ref, ref, sem, x_recv.at[0], {"tp": peers[0]}).wait_send()

    loads = {}
    loads["tokens"] = load(tokens_hbm, tokens, 12)
    barrier = pltpu.get_barrier_semaphore()
    for p in peers:
        pl.semaphore_signal(barrier, inc=1, device_id={"tp": p}, device_id_type=MESH)
    for i in range(1, NR):
        pl.semaphore_signal(
            barrier, inc=1, device_id={"ep": z * NR + mates[i]}, device_id_type=MESH
        )
    for i in (1, 2, 6, 7):
        pl.semaphore_signal(
            barrier, inc=1, device_id={"ep": planes[i] * NR + r}, device_id_type=MESH
        )

    loads["lengths"] = load(lengths_hbm, lengths, 13)
    loads["cum"] = load(cum_hbm, cum, 0)
    loads["chosen"] = load(chosen_hbm, chosen, 14)
    loads["route"] = load(route_hbm, route_weight, 15)
    loads["attn"] = load(attn_hbm, attn_gain, 16)
    loads["ffn"] = load(ffn_hbm, ffn_gain, 17)
    loads["mix"] = load(mix_hbm, mix_gate, 18)
    loads["bias"] = load(bias_hbm, forget_bias, 19)

    def kv_load(q):
        part = pl.ds(4 * q, 4)
        return pltpu.make_async_copy(kv_hbm.at[part], kv.at[part], kv_sem.at[q])

    for q in range(4):
        kv_load(q).start()
    loads["wk"] = load(wk_hbm, wkv.at[pl.ds(0, 64)], 1)
    loads["wv"] = load(wv_hbm, wkv.at[pl.ds(64, 64)], 2)
    loads["wf"] = load(wf_hbm, wf, 3)
    loads["wq"] = load(wq_hbm, wq, 4)
    loads["tokens"].wait()
    pl.semaphore_wait(barrier, 14)

    for p in peers:
        remote(tokens, xbuf.at[tp], x_send, x_recv.at[tp], {"tp": p}).start()
    for i in (2, 6):
        pl.semaphore_signal(
            ready_a, inc=1, device_id={"ep": planes[i] * NR + r}, device_id_type=MESH
        )
    xbuf[tp] = tokens[...]
    loads["wo"] = load(wo_hbm, wo, 5)
    loads["dg"] = load(dg_hbm, dg, 6)
    loads["du"] = load(du_hbm, du, 7)
    loads["dd"] = load(dd_hbm, dd, 8)
    loads["eg"] = load(eg_hbm, eg, 9)
    loads["eu"] = load(eu_hbm, eu, 10)
    loads["ed"] = load(ed_hbm, ed, 11)

    for name in ("lengths", "cum"):
        loads[name].wait()

    seq_row = iota((TOK, 1), 0)
    length = jnp.zeros((TOK, 1), jnp.int32)
    for i in range(TOK):
        length = jnp.where(seq_row == i, lengths[i], length)
    pos = iota((TOK, 1024), 1)
    for h in range(4):
        rows = cum[:, h, :]
        last = jnp.sum(jnp.where(pos == length - 1, rows, 0.0), axis=1, keepdims=True)
        rows = jnp.where(pos < length, last - rows, -jnp.inf)
        for q in range(4):
            gate[16 * q + 4 * h : 16 * q + 4 * h + 4, :] = rows[4 * q : 4 * q + 4]

    def key_part(q, carry):
        kv_load(q).wait()
        for i in range(4):
            turned = jnp.transpose(kv[4 * q + i])
            keys[q, 64 * i : 64 * i + 64, :] = turned[0:64]
        for i in range(2):
            s = 4 * q + 2 * i
            values[q, :, 128 * i : 128 * i + 128] = jnp.concatenate(
                [kv[s][:, HD:128], kv[s + 1][:, HD:128]], axis=1
            )
        return carry

    lax.fori_loop(0, 4, key_part, 0)

    pl.semaphore_wait(ready_a, 2)
    for i in range(1, NR):
        pl.semaphore_signal(
            ready_b, inc=1, device_id={"ep": z * NR + mates[i]}, device_id_type=MESH
        )

    for name in ("attn", "bias"):
        loads[name].wait()
    attn32[...] = attn_gain[...].astype(F32)
    for name in ("wk", "wv", "wf", "wq"):
        loads[name].wait()
    squares = jnp.zeros((TOK, 128), F32)
    query = jnp.zeros((TOK, 256), F32)
    kv_new = jnp.zeros((TOK, 128), F32)
    forget = jnp.zeros((TOK, 4), F32)
    for i in (0, 1, 3, 2):
        p = lax.rem(tp + i, NTP)
        if i:
            arrived(xbuf.at[p], x_recv.at[p])
        rows = xbuf[p].astype(F32)
        scaled = []
        for f in range(4):
            part = rows[:, 128 * f : 128 * f + 128]
            squares = squares + part * part
            scaled.append((part * attn32[pl.ds(4 * p + f, 1), :]).astype(BF16))
        scaled = jnp.concatenate(scaled, axis=1)
        span = pl.ds(pl.multiple_of(p * W, W), W)
        query = query + dot(scaled, wq[span, :])
        kv_new = kv_new + dot_nt(scaled, wkv[:, span])
        forget = forget + dot_nt(scaled, wf[:, span])
    root = lax.rsqrt(jnp.sum(squares, axis=1, keepdims=True) * (1.0 / 2048.0) + EPS)
    query = (query * root).astype(BF16)
    kv_new = (kv_new * root).astype(BF16)
    forget = forget * root
    head_lane = iota((TOK, 4), 1)
    bias = jnp.zeros((TOK, 4), F32)
    for h in range(4):
        bias = jnp.where(head_lane == h, forget_bias[h], bias)
    forget = forget + bias
    forget = jnp.minimum(forget, 0.0) - jnp.log1p(jnp.exp(-jnp.abs(forget)))

    low = iota((TOK, 128), 1) < HD
    heads = []
    for pair in (query[:, 0:128], query[:, 128:256]):
        pair = pair.astype(F32)
        other = pltpu.roll(pair, HD, 1)
        heads += [jnp.where(low, pair, other), jnp.where(low, other, pair)]
    def by_quad(per_head):
        return jnp.concatenate(
            [per_head[h][4 * q : 4 * q + 4] for q in range(4) for h in range(4)], axis=0
        )

    heads = by_quad(heads)
    kv64 = by_quad([kv_new.astype(F32)] * 4)
    f64 = by_quad([forget[:, h : h + 1] for h in range(4)])
    low64 = iota((64, 128), 1) < HD
    scale = HD ** (-0.5)
    own = jnp.sum(jnp.where(low64, heads * kv64, 0.0), axis=1, keepdims=True) * scale - f64
    mine_only = iota((64, 256), 1) // HD == iota((64, 256), 0) % 4
    blocks = jnp.where(mine_only, jnp.concatenate([heads] * 2, axis=1), 0.0).astype(BF16)
    score = jnp.concatenate(
        [dot(blocks[16 * q : 16 * q + 16], keys[q]) for q in range(4)], axis=0
    )
    score = score * scale + gate[...]
    highest = jnp.maximum(jnp.max(score, axis=1, keepdims=True), own)
    prob = jnp.exp(score - highest)
    own_prob = jnp.exp(own - highest)
    inverse = 1.0 / (jnp.sum(prob, axis=1, keepdims=True) + own_prob)
    prob = prob.astype(BF16)
    mixed_values = jnp.concatenate(
        [dot(prob[16 * q : 16 * q + 16], values[q]) for q in range(4)], axis=0
    )
    mixed_values = jnp.where(mine_only, mixed_values, 0.0)
    blended = mixed_values[:, 0:128] + mixed_values[:, 128:256]
    blended = blended + pltpu.roll(blended, HD, 1)
    value_row = jnp.where(low64, pltpu.roll(kv64, HD, 1), kv64)
    blended = (blended + own_prob * value_row) * inverse
    per_head = [
        jnp.concatenate(
            [blended[16 * q + 4 * h : 16 * q + 4 * h + 4] for q in range(4)], axis=0
        )
        for h in range(4)
    ]
    head_out = jnp.concatenate(
        [
            jnp.where(low, per_head[0], per_head[1]),
            jnp.where(low, per_head[2], per_head[3]),
        ],
        axis=1,
    ).astype(BF16)
    loads["wo"].wait()
    for p in peers:
        pbuf[p] = dot(head_out, wo[:, pl.ds(pl.multiple_of(p * W, W), W)]).astype(BF16)
        remote(pbuf.at[p], abuf.at[tp, p], p_send, p_recv.at[tp], {"tp": p}).start()
    pbuf[tp] = dot(head_out, wo[:, pl.ds(pl.multiple_of(tp * W, W), W)]).astype(BF16)
    for i in (1, 2, 3):
        for p in peers:
            q = lax.rem(p + i, NTP)
            remote(pbuf.at[q], abuf.at[tp, q], p_send, r_recv.at[tp], {"tp": p}).start()
    abuf[tp] = pbuf[...]

    for name in ("chosen", "route"):
        loads[name].wait()
    pick = chosen[...]
    expert = iota((NEP, TOK), 0)
    hot = [jnp.where(expert == pick[k : k + 1, :], 1.0, 0.0) for k in range(2)]
    earlier = one_hot(iota((TOK, TOK), 0) < iota((TOK, TOK), 1))
    before = dot((hot[0] + hot[1]).astype(BF16), earlier)
    away = lax.rem(pick // NR - z + NZ, NZ)
    order = jnp.where(away <= 4, jnp.maximum(2 * away - 1, 0), 16 - 2 * away)
    place = 2.0 * (order * NR + lax.rem(pick, NR)).astype(F32)
    slots = [
        place[k : k + 1, :] + jnp.sum(hot[k] * before, axis=0, keepdims=True)
        for k in range(2)
    ]
    weight = route_weight[...]
    w_rows = [three_parts(weight[k : k + 1, :]) for k in range(2)]
    info = jnp.concatenate(
        slots + [part.astype(F32) for k in range(2) for part in w_rows[k]], axis=0
    ).astype(BF16)
    spread = one_hot(iota((TOK, 64), 0) == iota((TOK, 64), 1) % TOK)
    spread_t = one_hot(iota((64, TOK), 0) % TOK == iota((64, TOK), 1))
    info_rows = dot(info, spread).astype(jnp.int32)
    info_cols = dot_nt(spread_t, info)
    row = iota((512, 64), 0)
    col_fb = iota((512, 64), 1) // TOK
    dmask = jnp.zeros((512, 64), F32)
    for k in range(2):
        dmask = dmask + jnp.where(row == info_rows[k : k + 1, :] * 4 + col_fb, 1.0, 0.0)
    dmat[...] = dmask.astype(BF16)
    for k in range(2):
        slot_col = info_cols[:, k : k + 1].astype(jnp.int32) * 4
        for ref, lo, n in ((rmat_n, 0, 8 * SN), (rmat_f, 8 * SN, 8 * SF)):
            lane = iota((64, n), 1) + lo
            row_fb = iota((64, n), 0) // TOK
            ref[pl.ds(64 * k, 64), :] = one_hot(lane == slot_col + row_fb)
    w_cols = [
        info_cols[:, 2 + 3 * k : 3 + 3 * k]
        + info_cols[:, 3 + 3 * k : 4 + 3 * k]
        + info_cols[:, 4 + 3 * k : 5 + 3 * k]
        for k in range(2)
    ]

    for n, ref, ref_t in ((SN, perm_n, permt_n), (SB, perm_b, permt_b), (NR, None, permt_c)):

        def perm_part(i, carry, n=n, ref=ref, ref_t=ref_t):
            base = 0 if n == NR else pl.multiple_of(64 * i, 64)
            a = iota((64, 8 * n), 0) + base
            b = iota((64, 8 * n), 1)
            if ref is not None:
                ref[pl.ds(base, 64), :] = one_hot(lax.rem(a, 2 * n) * 4 + a // (2 * n) == b)
            ref_t[pl.ds(base, 64), :] = one_hot(lax.rem(b, 2 * n) * 4 + b // (2 * n) == a)
            return carry

        if n > NR:
            lax.fori_loop(0, n // NR, perm_part, 0)
        else:
            perm_part(0, 0)

    for name in ("ffn", "mix"):
        loads[name].wait()
    ffn32[...] = ffn_gain[...].astype(F32)
    pl.semaphore_wait(ready_b, 7)

    for p in peers:
        arrived(abuf.at[p, tp], p_recv.at[p])
    def residual_of(q):
        attention = abuf[0, q].astype(F32)
        for p in range(1, NTP):
            attention = attention + abuf[p, q].astype(F32)
        return (xbuf[q].astype(F32) + attention).astype(BF16)

    residual = residual_of(tp)

    def stack(rows):
        return jnp.concatenate([rows[:, f * 128 : (f + 1) * 128] for f in range(4)], axis=0)

    def unstack(rows):
        return jnp.concatenate([rows[16 * f : 16 * f + 16] for f in range(4)], axis=1)

    def block(b):
        return ORDER.index((NZ - ORDER[b]) % NZ)

    def mine(b):
        return block(b) * NR + r

    outgoing = dot(dmat[pl.ds(8 * SD, 8 * SA), :], stack(residual))
    outg[...] = outgoing.reshape(SA, 8, 128).astype(BF16)
    for b in range(DIRECT, NZ):
        dz = ORDER[b]
        for i in range(1, NR + 1):
            m = mates[i % NR]
            remote(
                outg.at[(b - DIRECT) * NR + m],
                gath.at[tp, mine(b)],
                o_send,
                o_recv.at[block(b)],
                {"ep": planes[dz] * NR + m},
            ).start()
    for p in peers:
        arrived(abuf.at[p, pl.ds(0, 3)], r_recv.at[p])
    for q in range(NTP):
        rbuf[q] = residual_of(q)
    wide = jnp.concatenate([stack(rbuf[q]) for q in range(NTP)], axis=1)
    outgoing = dot(dmat[pl.ds(0, 8 * SD), :], wide)
    for q in range(NTP):
        outn[:, q] = outgoing[:, 128 * q : 128 * q + 128].reshape(SD, 8, 128).astype(BF16)
    for b in range(DIRECT):
        dz = ORDER[b]
        for i in range(1, NR + 1):
            if b or i < NR:
                m = mates[i % NR]
                remote(
                    outn.at[b * NR + m],
                    gath.at[:, mine(b)],
                    n_send,
                    o_recv.at[block(b)],
                    {"ep": planes[dz] * NR + m},
                ).start()
    gath[:, r] = outn[r]

    for b in range(DIRECT, NZ):
        chunk = gath.at[tp, pl.ds(b * NR, NR)]
        arrived(chunk, o_recv.at[b])
        for p in peers:
            remote(chunk, chunk, g_send, g_recv.at[tp], {"tp": p}).start()

    res_full = jnp.concatenate([rbuf[p] for p in range(NTP)], axis=1).astype(F32)
    square = jnp.mean(res_full * res_full, axis=1, keepdims=True)
    ffn_row = gain_row(ffn_gain)
    h_two = (res_full * lax.rsqrt(square + EPS) * ffn_row).astype(BF16)
    for name in ("dg", "du", "dd"):
        loads[name].wait()
    dense_act = (silu(dot(h_two, dg[...])) * dot(h_two, du[...])).astype(BF16)
    mixing = jnp.sum(h_two.astype(F32) * gain_row(mix_gate), axis=1, keepdims=True)
    blend = 1.0 / (1.0 + jnp.exp(-mixing))
    dpart[...] = dot(dense_act, dd[...]) * blend
    for name in ("eg", "eu", "ed"):
        loads[name].wait()

    def scaled_rows(rows, lo, n, c):
        start = c * 128 if isinstance(c, int) else pl.multiple_of(c * 128, 128)
        hbuf[2 * lo : 2 * (lo + n), pl.ds(start, 128)] = (rows * ffn32[pl.ds(c, 1), :]).astype(
            BF16
        )
        return rows * rows

    def root_of(squares):
        return lax.rsqrt(jnp.sum(squares, axis=1, keepdims=True) * (1.0 / 2048.0) + EPS)

    def direct_rows(lo, n, perm):
        wide = jnp.concatenate(
            [gath[q, pl.ds(lo, n)].reshape(8 * n, 128) for q in range(NTP)], axis=1
        )
        rows = dot(perm[...], wide)
        squares = jnp.zeros((2 * n, 128), F32)
        for q in range(NTP):
            for f in range(4):
                part = rows[2 * n * f : 2 * n * (f + 1), 128 * q : 128 * q + 128]
                squares = squares + scaled_rows(part, lo, n, 4 * q + f)
        return root_of(squares)

    def far_source(sources):
        wide = jnp.concatenate(
            [gath[p, pl.ds(SD, SA)].reshape(8 * SA, 128) for p in sources], axis=1
        )
        rows = dot(perm_n[...], wide)
        squares = jnp.zeros((2 * SA, 128), F32)
        gate_pre = jnp.zeros((2 * SA, 256), F32)
        up_pre = jnp.zeros((2 * SA, 256), F32)
        for k, p in enumerate(sources):
            for f in range(4):
                part = rows[2 * SA * f : 2 * SA * (f + 1), 128 * k : 128 * k + 128]
                squares = squares + scaled_rows(part, SD, SA, 4 * p + f)
        for p in sources:
            span = pl.ds(pl.multiple_of(p * W, W), W)
            hidden = hbuf[2 * SD : 128, span]
            gate_pre = gate_pre + dot(hidden, eg[span, :])
            up_pre = up_pre + dot(hidden, eu[span, :])
        return squares, gate_pre, up_pre

    far = far_source([tp])
    for b in range(DIRECT):
        lo = 0 if b else 1
        arrived(gath.at[:, pl.ds(b * NR + lo, NR - lo)], o_recv.at[b])
    root_n = direct_rows(0, SN, perm_n)
    root_b = direct_rows(SN, SB, perm_b)
    root = jnp.concatenate([root_n, root_b], axis=0)
    hidden = hbuf[0 : 2 * SD]
    act_d = silu(dot(hidden, eg[...]) * root) * (dot(hidden, eu[...]) * root)
    act_d = act_d.astype(BF16)
    act_b = act_d[2 * SN : 2 * SD]
    part = pl.ds(0, 2 * SB)
    for p in peers:
        ysend[p, part] = dot(act_b, ed[:, pl.ds(pl.multiple_of(p * W, W), W)]).astype(BF16)
        remote(
            ysend.at[p, part], ybuf.at[tp, part], y_send, y_recv.at[0, tp], {"tp": p}
        ).start()
    sides = [lax.rem(tp + 1, NTP), lax.rem(tp + 3, NTP)]
    for p in sides:
        arrived(gath.at[p, pl.ds(SD, SA)], g_recv.at[p])
    far = [a + b for a, b in zip(far, far_source(sides))]
    arrived(gath.at[peers[0], pl.ds(SD, SA)], g_recv.at[peers[0]])
    squares, gate_pre, up_pre = [a + b for a, b in zip(far, far_source(peers[:1]))]
    root_a = root_of(squares)
    act_f = (silu(gate_pre * root_a) * (up_pre * root_a)).astype(BF16)
    for half, lo, n in ((2, 32, NR), (1, 16, SB)):
        part = pl.ds(2 * lo, 2 * n)
        for p in peers:
            if half == 2:
                ysend[p, pl.ds(2 * SB, 2 * SA)] = dot(
                    act_f, ed[:, pl.ds(pl.multiple_of(p * W, W), W)]
                ).astype(BF16)
            remote(
                ysend.at[p, part], ybuf.at[tp, part], y_send, y_recv.at[half, tp], {"tp": p}
            ).start()
    act_n = act_d[0 : 2 * SN]
    part = dot(act_n, ed[...]).astype(BF16)
    wide = jnp.concatenate([stack(part[:, q * W : (q + 1) * W]) for q in range(NTP)], axis=1)
    turned = dot(permt_n[...], wide)
    for q in range(NTP):
        routn[:, q] = turned[:, 128 * q : 128 * q + 128].reshape(SN, 8, 128).astype(BF16)
    for b in range(NEAR):
        dz = ORDER[b]
        for i in range(1, NR + 1):
            if b or i < NR:
                m = mates[i % NR]
                remote(
                    routn.at[b * NR + m],
                    rinn.at[mine(b)],
                    c_send,
                    c_recv,
                    {"ep": planes[dz] * NR + m},
                ).start()
    rinn[r] = routn[r]

    own_cols = ed[:, pl.ds(pl.multiple_of(tp * W, W), W)]
    sum_b = dot(act_b, own_cols).astype(BF16).astype(F32)
    sum_a = dot(act_f, own_cols).astype(BF16).astype(F32)
    for half, lo, n, turn, first, last, rows in (
        (0, 0, SB, permt_b, 3, 5, sum_b),
        (2, 32, NR, permt_c, 7, 8, sum_a[32:48]),
        (1, 16, SB, permt_b, 5, 7, sum_a[0:32]),
    ):
        for p in peers:
            part = pl.ds(2 * lo, 2 * n)
            arrived(ybuf.at[p, part], y_recv.at[half, p])
            rows = rows + ybuf[p, part].astype(F32)
        turned = dot(turn[...], stack(rows.astype(BF16)))
        rout[pl.ds(lo, n)] = turned.reshape(n, 8, 128).astype(BF16)
        for b in reversed(range(first, last)):
            dz = ORDER[b]
            for i in range(1, NR + 1):
                m = mates[i % NR]
                remote(
                    rout.at[(b - NEAR) * NR + m],
                    rin.at[mine(b) - SN],
                    b_send,
                    b_recv,
                    {"ep": planes[dz] * NR + m},
                ).start()

    def routed(picked):
        return unstack(picked[0:64] * w_cols[0] + picked[64:128] * w_cols[1])

    arrived(rinn.at[pl.ds(0, SN - 1)], c_recv)
    wide = jnp.concatenate([rinn[:, q].reshape(8 * SN, 128) for q in range(NTP)], axis=1)
    picked = dot(rmat_n[...], wide)
    for q in range(NTP):
        part = routed(picked[:, 128 * q : 128 * q + 128])
        dpart[:, q * W : (q + 1) * W] = part + dpart[:, q * W : (q + 1) * W]
    for i in (2, 1, 3, 0):
        q = lax.rem(tp + i, NTP)
        part = dpart[:, pl.ds(pl.multiple_of(q * W, W), W)]
        if i:
            dsend[q] = part.astype(BF16)
            remote(dsend.at[q], dbuf.at[tp], d_send, d_recv.at[tp], {"tp": q}).start()
        else:
            mixed = residual.astype(F32) + part

    arrived(rin, b_recv)
    mixed = mixed + routed(dot(rmat_f[...], rin[...].reshape(8 * SF, 128)))
    for p in peers:
        arrived(dbuf.at[p], d_recv.at[p])
        mixed = mixed + dbuf[p].astype(F32)
    out[...] = mixed.astype(BF16)

    left(xbuf.at[pl.ds(0, 3)], x_send)
    left(abuf.at[pl.ds(0, 3)], p_send)
    left(outg, o_send)
    left(outn.at[pl.ds(0, SD - 1)], n_send)
    left(gath.at[pl.ds(0, 3), pl.ds(SD, SA)], g_send)
    left(dsend.at[pl.ds(0, 3)], d_send)
    left(ysend.at[pl.ds(0, 3)], y_send)
    left(rout, b_send)
    left(routn.at[pl.ds(0, SN - 1)], c_send)


def local(
    tokens,
    kv_cache,
    cum_gate,
    lengths,
    w_query,
    w_key,
    w_value,
    w_forget,
    forget_bias,
    w_out,
    attn_gain,
    ffn_gain,
    mix_gate,
    expert_gate,
    expert_up,
    expert_down,
    chosen,
    route_weight,
    dense_gate,
    dense_up,
    dense_down,
):
    vmem = pl.BlockSpec(memory_space=pltpu.VMEM)
    hbm = pl.BlockSpec(memory_space=ANY)
    dma = pltpu.SemaphoreType.DMA
    regular = pltpu.SemaphoreType.REGULAR
    scratch = [
        pltpu.VMEM((TOK, W), BF16),
        pltpu.SMEM((TOK,), jnp.int32),
        pltpu.SMEM((4,), F32),
        pltpu.VMEM((16, 128), BF16),
        pltpu.VMEM((16, 128), BF16),
        pltpu.VMEM((16, 128), BF16),
        pltpu.VMEM((2, TOK), jnp.int32),
        pltpu.VMEM((2, TOK), F32),
        pltpu.VMEM((TOK, 1024, 128), BF16),
        pltpu.VMEM((4, 256, 1024), BF16),
        pltpu.VMEM((4, 1024, 256), BF16),
        pltpu.VMEM((TOK, 4, 1024), F32),
        pltpu.VMEM((2048, 256), BF16),
        pltpu.VMEM((128, 2048), BF16),
        pltpu.VMEM((4, 2048), BF16),
        pltpu.VMEM((256, 2048), BF16),
        pltpu.VMEM((2048, 256), BF16),
        pltpu.VMEM((2048, 256), BF16),
        pltpu.VMEM((256, 2048), BF16),
        pltpu.VMEM((2048, 256), BF16),
        pltpu.VMEM((2048, 256), BF16),
        pltpu.VMEM((256, 2048), BF16),
        pltpu.VMEM((NTP, TOK, W), BF16),
        pltpu.VMEM((64, 1024), F32),
        pltpu.VMEM((NTP, TOK, W), BF16),
        pltpu.VMEM((NTP, NTP, TOK, W), BF16),
        pltpu.VMEM((512, 64), BF16),
        pltpu.VMEM((128, 8 * SN), BF16),
        pltpu.VMEM((128, 8 * SF), BF16),
        pltpu.VMEM((8 * SN, 8 * SN), BF16),
        pltpu.VMEM((8 * SN, 8 * SN), BF16),
        pltpu.VMEM((8 * SB, 8 * SB), BF16),
        pltpu.VMEM((8 * SB, 8 * SB), BF16),
        pltpu.VMEM((64, 64), BF16),
        pltpu.VMEM((NTP, TOK, W), BF16),
        pltpu.VMEM((SA, 8, 128), BF16),
        pltpu.VMEM((SD, NTP, 8, 128), BF16),
        pltpu.VMEM((NTP, NEP, 8, 128), BF16),
        pltpu.VMEM((128, 2048), BF16),
        pltpu.VMEM((TOK, 2048), F32),
        pltpu.VMEM((NTP, TOK, W), BF16),
        pltpu.VMEM((NTP, TOK, W), BF16),
        pltpu.VMEM((NTP, 2 * SF, W), BF16),
        pltpu.VMEM((NTP, 2 * SF, W), BF16),
        pltpu.VMEM((SF, 8, 128), BF16),
        pltpu.VMEM((SN, NTP, 8, 128), BF16),
        pltpu.VMEM((SF, 8, 128), BF16),
        pltpu.VMEM((SN, NTP, 8, 128), BF16),
        pltpu.VMEM((16, 128), F32),
        pltpu.VMEM((16, 128), F32),
        dma((20,)),
        dma((4,)),
        dma,
        dma((NTP,)),
        regular,
        regular,
        dma,
        dma((NTP,)),
        dma((NTP,)),
        dma,
        dma((NZ,)),
        dma,
        dma((NTP,)),
        dma,
        dma((NTP,)),
        dma,
        dma((3, NTP)),
        dma,
        dma,
        dma,
        dma,
        dma,
    ]
    return pl.pallas_call(
        layer,
        out_shape=pltpu.VMEM((TOK, W), BF16),
        in_specs=[hbm] * 21,
        out_specs=vmem,
        scratch_shapes=scratch,
        compiler_params=pltpu.CompilerParams(collective_id=0, has_side_effects=True),
        name="layer",
    )(
        tokens,
        lengths,
        forget_bias,
        attn_gain.reshape(16, 128),
        ffn_gain.reshape(16, 128),
        mix_gate.reshape(16, 128),
        chosen.T,
        route_weight.T,
        kv_cache,
        cum_gate,
        w_query,
        w_key.T,
        w_value.T,
        w_forget.T,
        w_out,
        expert_gate[0],
        expert_up[0],
        expert_down[0],
        dense_gate,
        dense_up,
        dense_down,
    )


def solution(mesh):
    in_specs = (
        P("ep", "tp"),
        P("ep", None, "tp"),
        P("ep", "tp", None),
        P("ep"),
        P(None, "tp"),
        P(None, "tp"),
        P(None, "tp"),
        P(None, "tp"),
        P("tp"),
        P("tp", None),
        P(),
        P(),
        P(),
        P("ep", None, "tp"),
        P("ep", None, "tp"),
        P("ep", "tp", None),
        P("ep", None),
        P("ep", None),
        P(None, "tp"),
        P(None, "tp"),
        P("tp", None),
    )
    out_specs = P("ep", "tp")
    return jax.shard_map(local, mesh=mesh, in_specs=in_specs, out_specs=out_specs, check_vma=False)
```

```python
import jax
import jax.numpy as jnp
from jax import lax
from jax.experimental import pallas as pl
from jax.experimental.pallas import tpu as pltpu
from jax.sharding import PartitionSpec as P

EPS = 1e-06
F32 = jnp.float32
BF16 = jnp.bfloat16
MESH = pl.DeviceIdType.MESH
ANY = pl.ANY

TOK = 16
HD = 64
NTP = 4
NZ = 8
NR = 8
NEP = 64
W = 512
NEAR = 3
DIRECT = 5
SD = DIRECT * NR
SN = NEAR * NR
SF = NEP - SN
SB = 16
SA = SF - SB
ORDER = (0, 1, 7, 2, 6, 3, 5, 4)
NT = (((1,), (1,)), ((), ()))


def iota(shape, dim):
    return lax.broadcasted_iota(jnp.int32, shape, dim)


def dot(a, b):
    return jnp.dot(a, b, preferred_element_type=F32)


def dot_nt(a, b):
    return lax.dot_general(a, b, NT, preferred_element_type=F32)


def one_hot(mask):
    return jnp.where(mask, 1.0, 0.0).astype(BF16)


def three_parts(a):
    hi = a.astype(BF16)
    rest = a - hi.astype(F32)
    mid = rest.astype(BF16)
    low = (rest - mid.astype(F32)).astype(BF16)
    return hi, mid, low


def gain_row(gain_ref):
    gain = gain_ref[...].astype(F32)
    return jnp.concatenate([gain[j : j + 1, :] for j in range(16)], axis=1)


def silu(a):
    return a * (1.0 / (1.0 + jnp.exp(-a)))


def layer(
    tokens_hbm,
    lengths_hbm,
    bias_hbm,
    attn_hbm,
    ffn_hbm,
    mix_hbm,
    chosen_hbm,
    route_hbm,
    kv_hbm,
    cum_hbm,
    wq_hbm,
    wk_hbm,
    wv_hbm,
    wf_hbm,
    wo_hbm,
    eg_hbm,
    eu_hbm,
    ed_hbm,
    dg_hbm,
    du_hbm,
    dd_hbm,
    out,
    tokens,
    lengths,
    forget_bias,
    attn_gain,
    ffn_gain,
    mix_gate,
    chosen,
    route_weight,
    kv,
    keys,
    values,
    cum,
    wq,
    wkv,
    wf,
    wo,
    eg,
    eu,
    ed,
    dg,
    du,
    dd,
    xbuf,
    gate,
    pbuf,
    abuf,
    dmat,
    rmat_n,
    rmat_b,
    rmat_f,
    perm_n,
    permt_n,
    perm_b,
    permt_b,
    permt_c,
    rbuf,
    outg,
    outn,
    gath,
    hbuf,
    dpart,
    dsend,
    dbuf,
    ysend,
    ybuf,
    rout,
    routn,
    rin,
    rinn,
    ffn32,
    attn32,
    load_sem,
    kv_sem,
    x_send,
    x_recv,
    ready_a,
    ready_b,
    p_send,
    p_recv,
    r_recv,
    o_send,
    o_recv,
    g_send,
    g_recv,
    d_send,
    d_recv,
    y_send,
    y_recv,
    b_send,
    b_recv,
    n_send,
    c_send,
    c_recv,
):
    ep = lax.axis_index("ep")
    tp = lax.axis_index("tp")
    z = ep // NR
    r = lax.rem(ep, NR)
    peers = [lax.rem(tp + i, NTP) for i in (2, 1, 3)]
    planes = [lax.rem(z + i, NZ) for i in range(NZ)]
    mates = [lax.rem(r + i, NR) for i in range(NR)]

    def load(src, dst, i):
        copy = pltpu.make_async_copy(src, dst, load_sem.at[i])
        copy.start()
        return copy

    def remote(src, dst, send, recv, device):
        return pltpu.make_async_remote_copy(
            src_ref=src,
            dst_ref=dst,
            send_sem=send,
            recv_sem=recv,
            device_id=device,
            device_id_type=MESH,
        )

    def arrived(ref, sem):
        remote(ref, ref, x_send, sem, {"tp": peers[0]}).wait_recv()

    def left(ref, sem):
        remote(ref, ref, sem, x_recv.at[0], {"tp": peers[0]}).wait_send()

    loads = {}
    loads["tokens"] = load(tokens_hbm, tokens, 12)
    barrier = pltpu.get_barrier_semaphore()
    for p in peers:
        pl.semaphore_signal(barrier, inc=1, device_id={"tp": p}, device_id_type=MESH)
    for i in range(1, NR):
        pl.semaphore_signal(
            barrier, inc=1, device_id={"ep": z * NR + mates[i]}, device_id_type=MESH
        )
    for i in (1, 2, 6, 7):
        pl.semaphore_signal(
            barrier, inc=1, device_id={"ep": planes[i] * NR + r}, device_id_type=MESH
        )

    loads["lengths"] = load(lengths_hbm, lengths, 13)
    loads["cum"] = load(cum_hbm, cum, 0)
    loads["chosen"] = load(chosen_hbm, chosen, 14)
    loads["route"] = load(route_hbm, route_weight, 15)
    loads["attn"] = load(attn_hbm, attn_gain, 16)
    loads["ffn"] = load(ffn_hbm, ffn_gain, 17)
    loads["mix"] = load(mix_hbm, mix_gate, 18)
    loads["bias"] = load(bias_hbm, forget_bias, 19)

    def kv_load(q):
        part = pl.ds(4 * q, 4)
        return pltpu.make_async_copy(kv_hbm.at[part], kv.at[part], kv_sem.at[q])

    for q in range(4):
        kv_load(q).start()
    loads["wk"] = load(wk_hbm, wkv.at[pl.ds(0, 64)], 1)
    loads["wv"] = load(wv_hbm, wkv.at[pl.ds(64, 64)], 2)
    loads["wf"] = load(wf_hbm, wf, 3)
    loads["wq"] = load(wq_hbm, wq, 4)
    loads["tokens"].wait()
    pl.semaphore_wait(barrier, 14)

    for p in peers:
        remote(tokens, xbuf.at[tp], x_send, x_recv.at[tp], {"tp": p}).start()
    for i in (2, 6):
        pl.semaphore_signal(
            ready_a, inc=1, device_id={"ep": planes[i] * NR + r}, device_id_type=MESH
        )
    xbuf[tp] = tokens[...]
    loads["wo"] = load(wo_hbm, wo, 5)
    loads["dg"] = load(dg_hbm, dg, 6)
    loads["du"] = load(du_hbm, du, 7)
    loads["dd"] = load(dd_hbm, dd, 8)
    loads["eg"] = load(eg_hbm, eg, 9)
    loads["eu"] = load(eu_hbm, eu, 10)
    loads["ed"] = load(ed_hbm, ed, 11)

    for name in ("lengths", "cum"):
        loads[name].wait()

    seq_row = iota((TOK, 1), 0)
    length = jnp.zeros((TOK, 1), jnp.int32)
    for i in range(TOK):
        length = jnp.where(seq_row == i, lengths[i], length)
    pos = iota((TOK, 1024), 1)
    for h in range(4):
        rows = cum[:, h, :]
        last = jnp.sum(jnp.where(pos == length - 1, rows, 0.0), axis=1, keepdims=True)
        rows = jnp.where(pos < length, last - rows, -jnp.inf)
        for q in range(4):
            gate[16 * q + 4 * h : 16 * q + 4 * h + 4, :] = rows[4 * q : 4 * q + 4]

    def key_part(q, carry):
        kv_load(q).wait()
        for i in range(4):
            turned = jnp.transpose(kv[4 * q + i])
            keys[q, 64 * i : 64 * i + 64, :] = turned[0:64]
        for i in range(2):
            s = 4 * q + 2 * i
            values[q, :, 128 * i : 128 * i + 128] = jnp.concatenate(
                [kv[s][:, HD:128], kv[s + 1][:, HD:128]], axis=1
            )
        return carry

    lax.fori_loop(0, 4, key_part, 0)

    pl.semaphore_wait(ready_a, 2)
    for i in range(1, NR):
        pl.semaphore_signal(
            ready_b, inc=1, device_id={"ep": z * NR + mates[i]}, device_id_type=MESH
        )

    for name in ("attn", "bias"):
        loads[name].wait()
    attn32[...] = attn_gain[...].astype(F32)
    for name in ("wk", "wv", "wf", "wq"):
        loads[name].wait()
    squares = jnp.zeros((TOK, 128), F32)
    query = jnp.zeros((TOK, 256), F32)
    kv_new = jnp.zeros((TOK, 128), F32)
    forget = jnp.zeros((TOK, 4), F32)
    for i in (0, 1, 3, 2):
        p = lax.rem(tp + i, NTP)
        if i:
            arrived(xbuf.at[p], x_recv.at[p])
        rows = xbuf[p].astype(F32)
        scaled = []
        for f in range(4):
            part = rows[:, 128 * f : 128 * f + 128]
            squares = squares + part * part
            scaled.append((part * attn32[pl.ds(4 * p + f, 1), :]).astype(BF16))
        scaled = jnp.concatenate(scaled, axis=1)
        span = pl.ds(pl.multiple_of(p * W, W), W)
        query = query + dot(scaled, wq[span, :])
        kv_new = kv_new + dot_nt(scaled, wkv[:, span])
        forget = forget + dot_nt(scaled, wf[:, span])
    root = lax.rsqrt(jnp.sum(squares, axis=1, keepdims=True) * (1.0 / 2048.0) + EPS)
    query = (query * root).astype(BF16)
    kv_new = (kv_new * root).astype(BF16)
    forget = forget * root
    head_lane = iota((TOK, 4), 1)
    bias = jnp.zeros((TOK, 4), F32)
    for h in range(4):
        bias = jnp.where(head_lane == h, forget_bias[h], bias)
    forget = forget + bias
    forget = jnp.minimum(forget, 0.0) - jnp.log1p(jnp.exp(-jnp.abs(forget)))

    low = iota((TOK, 128), 1) < HD
    heads = []
    for pair in (query[:, 0:128], query[:, 128:256]):
        pair = pair.astype(F32)
        other = pltpu.roll(pair, HD, 1)
        heads += [jnp.where(low, pair, other), jnp.where(low, other, pair)]
    def by_quad(per_head):
        return jnp.concatenate(
            [per_head[h][4 * q : 4 * q + 4] for q in range(4) for h in range(4)], axis=0
        )

    heads = by_quad(heads)
    kv64 = by_quad([kv_new.astype(F32)] * 4)
    f64 = by_quad([forget[:, h : h + 1] for h in range(4)])
    low64 = iota((64, 128), 1) < HD
    scale = HD ** (-0.5)
    own = jnp.sum(jnp.where(low64, heads * kv64, 0.0), axis=1, keepdims=True) * scale - f64
    mine_only = iota((64, 256), 1) // HD == iota((64, 256), 0) % 4
    blocks = jnp.where(mine_only, jnp.concatenate([heads] * 2, axis=1), 0.0).astype(BF16)
    score = jnp.concatenate(
        [dot(blocks[16 * q : 16 * q + 16], keys[q]) for q in range(4)], axis=0
    )
    score = score * scale + gate[...]
    highest = jnp.maximum(jnp.max(score, axis=1, keepdims=True), own)
    prob = jnp.exp(score - highest)
    own_prob = jnp.exp(own - highest)
    inverse = 1.0 / (jnp.sum(prob, axis=1, keepdims=True) + own_prob)
    prob = prob.astype(BF16)
    mixed_values = jnp.concatenate(
        [dot(prob[16 * q : 16 * q + 16], values[q]) for q in range(4)], axis=0
    )
    mixed_values = jnp.where(mine_only, mixed_values, 0.0)
    blended = mixed_values[:, 0:128] + mixed_values[:, 128:256]
    blended = blended + pltpu.roll(blended, HD, 1)
    value_row = jnp.where(low64, pltpu.roll(kv64, HD, 1), kv64)
    blended = (blended + own_prob * value_row) * inverse
    per_head = [
        jnp.concatenate(
            [blended[16 * q + 4 * h : 16 * q + 4 * h + 4] for q in range(4)], axis=0
        )
        for h in range(4)
    ]
    head_out = jnp.concatenate(
        [
            jnp.where(low, per_head[0], per_head[1]),
            jnp.where(low, per_head[2], per_head[3]),
        ],
        axis=1,
    ).astype(BF16)
    loads["wo"].wait()
    for p in peers:
        pbuf[p] = dot(head_out, wo[:, pl.ds(pl.multiple_of(p * W, W), W)]).astype(BF16)
        remote(pbuf.at[p], abuf.at[tp, p], p_send, p_recv.at[tp], {"tp": p}).start()
    pbuf[tp] = dot(head_out, wo[:, pl.ds(pl.multiple_of(tp * W, W), W)]).astype(BF16)
    for i in (1, 2, 3):
        for p in peers:
            q = lax.rem(p + i, NTP)
            remote(pbuf.at[q], abuf.at[tp, q], p_send, r_recv.at[tp], {"tp": p}).start()
    abuf[tp] = pbuf[...]

    for name in ("chosen", "route"):
        loads[name].wait()
    pick = chosen[...]
    expert = iota((NEP, TOK), 0)
    hot = [jnp.where(expert == pick[k : k + 1, :], 1.0, 0.0) for k in range(2)]
    earlier = one_hot(iota((TOK, TOK), 0) < iota((TOK, TOK), 1))
    before = dot((hot[0] + hot[1]).astype(BF16), earlier)
    away = lax.rem(pick // NR - z + NZ, NZ)
    order = jnp.where(away <= 4, jnp.maximum(2 * away - 1, 0), 16 - 2 * away)
    place = 2.0 * (order * NR + lax.rem(pick, NR)).astype(F32)
    slots = [
        place[k : k + 1, :] + jnp.sum(hot[k] * before, axis=0, keepdims=True)
        for k in range(2)
    ]
    weight = route_weight[...]
    w_rows = [three_parts(weight[k : k + 1, :]) for k in range(2)]
    info = jnp.concatenate(
        slots + [part.astype(F32) for k in range(2) for part in w_rows[k]], axis=0
    ).astype(BF16)
    spread = one_hot(iota((TOK, 64), 0) == iota((TOK, 64), 1) % TOK)
    spread_t = one_hot(iota((64, TOK), 0) % TOK == iota((64, TOK), 1))
    info_rows = dot(info, spread).astype(jnp.int32)
    info_cols = dot_nt(spread_t, info)
    row = iota((512, 64), 0)
    col_fb = iota((512, 64), 1) // TOK
    dmask = jnp.zeros((512, 64), F32)
    for k in range(2):
        dmask = dmask + jnp.where(row == info_rows[k : k + 1, :] * 4 + col_fb, 1.0, 0.0)
    dmat[...] = dmask.astype(BF16)
    for k in range(2):
        slot_col = info_cols[:, k : k + 1].astype(jnp.int32) * 4
        for ref, lo, n in (
            (rmat_n, 0, 8 * SN),
            (rmat_b, 8 * SN, 8 * SB),
            (rmat_f, 8 * SD, 8 * SA),
        ):
            lane = iota((64, n), 1) + lo
            row_fb = iota((64, n), 0) // TOK
            ref[pl.ds(64 * k, 64), :] = one_hot(lane == slot_col + row_fb)
    w_cols = [
        info_cols[:, 2 + 3 * k : 3 + 3 * k]
        + info_cols[:, 3 + 3 * k : 4 + 3 * k]
        + info_cols[:, 4 + 3 * k : 5 + 3 * k]
        for k in range(2)
    ]

    for n, ref, ref_t in ((SN, perm_n, permt_n), (SB, perm_b, permt_b), (NR, None, permt_c)):

        def perm_part(i, carry, n=n, ref=ref, ref_t=ref_t):
            base = 0 if n == NR else pl.multiple_of(64 * i, 64)
            a = iota((64, 8 * n), 0) + base
            b = iota((64, 8 * n), 1)
            if ref is not None:
                ref[pl.ds(base, 64), :] = one_hot(lax.rem(a, 2 * n) * 4 + a // (2 * n) == b)
            ref_t[pl.ds(base, 64), :] = one_hot(lax.rem(b, 2 * n) * 4 + b // (2 * n) == a)
            return carry

        if n > NR:
            lax.fori_loop(0, n // NR, perm_part, 0)
        else:
            perm_part(0, 0)

    for name in ("ffn", "mix"):
        loads[name].wait()
    ffn32[...] = ffn_gain[...].astype(F32)
    pl.semaphore_wait(ready_b, 7)

    for p in peers:
        arrived(abuf.at[p, tp], p_recv.at[p])
    def residual_of(q):
        attention = abuf[0, q].astype(F32)
        for p in range(1, NTP):
            attention = attention + abuf[p, q].astype(F32)
        return (xbuf[q].astype(F32) + attention).astype(BF16)

    residual = residual_of(tp)

    def stack(rows):
        return jnp.concatenate([rows[:, f * 128 : (f + 1) * 128] for f in range(4)], axis=0)

    def unstack(rows):
        return jnp.concatenate([rows[16 * f : 16 * f + 16] for f in range(4)], axis=1)

    def block(b):
        return ORDER.index((NZ - ORDER[b]) % NZ)

    def mine(b):
        return block(b) * NR + r

    outgoing = dot(dmat[pl.ds(8 * SD, 8 * SA), :], stack(residual))
    outg[...] = outgoing.reshape(SA, 8, 128).astype(BF16)
    for b in range(DIRECT, NZ):
        dz = ORDER[b]
        for i in range(1, NR + 1):
            m = mates[i % NR]
            remote(
                outg.at[(b - DIRECT) * NR + m],
                gath.at[tp, mine(b)],
                o_send,
                o_recv.at[block(b)],
                {"ep": planes[dz] * NR + m},
            ).start()
    for p in peers:
        arrived(abuf.at[p, pl.ds(0, 3)], r_recv.at[p])
    for q in range(NTP):
        rbuf[q] = residual_of(q)
    wide = jnp.concatenate([stack(rbuf[q]) for q in range(NTP)], axis=1)
    outgoing = dot(dmat[pl.ds(0, 8 * SD), :], wide)
    for q in range(NTP):
        outn[:, q] = outgoing[:, 128 * q : 128 * q + 128].reshape(SD, 8, 128).astype(BF16)
    for b in range(DIRECT):
        dz = ORDER[b]
        for i in range(1, NR + 1):
            if b or i < NR:
                m = mates[i % NR]
                remote(
                    outn.at[b * NR + m],
                    gath.at[:, mine(b)],
                    n_send,
                    o_recv.at[block(b)],
                    {"ep": planes[dz] * NR + m},
                ).start()
    gath[:, r] = outn[r]

    for b in range(DIRECT, NZ):
        chunk = gath.at[tp, pl.ds(b * NR, NR)]
        arrived(chunk, o_recv.at[b])
        for p in peers:
            remote(chunk, chunk, g_send, g_recv.at[tp], {"tp": p}).start()

    res_full = jnp.concatenate([rbuf[p] for p in range(NTP)], axis=1).astype(F32)
    square = jnp.mean(res_full * res_full, axis=1, keepdims=True)
    ffn_row = gain_row(ffn_gain)
    h_two = (res_full * lax.rsqrt(square + EPS) * ffn_row).astype(BF16)
    for name in ("dg", "du", "dd"):
        loads[name].wait()
    dense_act = (silu(dot(h_two, dg[...])) * dot(h_two, du[...])).astype(BF16)
    mixing = jnp.sum(h_two.astype(F32) * gain_row(mix_gate), axis=1, keepdims=True)
    blend = 1.0 / (1.0 + jnp.exp(-mixing))
    dpart[...] = dot(dense_act, dd[...]) * blend
    for name in ("eg", "eu", "ed"):
        loads[name].wait()

    def scaled_rows(rows, lo, n, c):
        start = c * 128 if isinstance(c, int) else pl.multiple_of(c * 128, 128)
        hbuf[2 * lo : 2 * (lo + n), pl.ds(start, 128)] = (rows * ffn32[pl.ds(c, 1), :]).astype(
            BF16
        )
        return rows * rows

    def root_of(squares):
        return lax.rsqrt(jnp.sum(squares, axis=1, keepdims=True) * (1.0 / 2048.0) + EPS)

    def direct_rows(lo, n, perm):
        wide = jnp.concatenate(
            [gath[q, pl.ds(lo, n)].reshape(8 * n, 128) for q in range(NTP)], axis=1
        )
        rows = dot(perm[...], wide)
        squares = jnp.zeros((2 * n, 128), F32)
        for q in range(NTP):
            for f in range(4):
                part = rows[2 * n * f : 2 * n * (f + 1), 128 * q : 128 * q + 128]
                squares = squares + scaled_rows(part, lo, n, 4 * q + f)
        return root_of(squares)

    def far_source(sources):
        wide = jnp.concatenate(
            [gath[p, pl.ds(SD, SA)].reshape(8 * SA, 128) for p in sources], axis=1
        )
        rows = dot(perm_n[...], wide)
        squares = jnp.zeros((2 * SA, 128), F32)
        gate_pre = jnp.zeros((2 * SA, 256), F32)
        up_pre = jnp.zeros((2 * SA, 256), F32)
        for k, p in enumerate(sources):
            for f in range(4):
                part = rows[2 * SA * f : 2 * SA * (f + 1), 128 * k : 128 * k + 128]
                squares = squares + scaled_rows(part, SD, SA, 4 * p + f)
        for p in sources:
            span = pl.ds(pl.multiple_of(p * W, W), W)
            hidden = hbuf[2 * SD : 128, span]
            gate_pre = gate_pre + dot(hidden, eg[span, :])
            up_pre = up_pre + dot(hidden, eu[span, :])
        return squares, gate_pre, up_pre

    far = far_source([tp])
    for b in range(DIRECT):
        lo = 0 if b else 1
        arrived(gath.at[:, pl.ds(b * NR + lo, NR - lo)], o_recv.at[b])
    root_n = direct_rows(0, SN, perm_n)
    root_b = direct_rows(SN, SB, perm_b)
    root = jnp.concatenate([root_n, root_b], axis=0)
    hidden = hbuf[0 : 2 * SD]
    act_d = silu(dot(hidden, eg[...]) * root) * (dot(hidden, eu[...]) * root)
    act_d = act_d.astype(BF16)
    act_b = act_d[2 * SN : 2 * SD]
    part = pl.ds(0, 2 * SB)
    for p in peers:
        ysend[p, part] = dot(act_b, ed[:, pl.ds(pl.multiple_of(p * W, W), W)]).astype(BF16)
        remote(
            ysend.at[p, part], ybuf.at[tp, part], y_send, y_recv.at[0, tp], {"tp": p}
        ).start()
    sides = [lax.rem(tp + 1, NTP), lax.rem(tp + 3, NTP)]
    for p in sides:
        arrived(gath.at[p, pl.ds(SD, SA)], g_recv.at[p])
    far = [a + b for a, b in zip(far, far_source(sides))]
    arrived(gath.at[peers[0], pl.ds(SD, SA)], g_recv.at[peers[0]])
    squares, gate_pre, up_pre = [a + b for a, b in zip(far, far_source(peers[:1]))]
    root_a = root_of(squares)
    act_f = (silu(gate_pre * root_a) * (up_pre * root_a)).astype(BF16)
    for half, lo, n in ((2, 32, NR), (1, 16, SB)):
        part = pl.ds(2 * lo, 2 * n)
        for p in peers:
            if half == 2:
                ysend[p, pl.ds(2 * SB, 2 * SA)] = dot(
                    act_f, ed[:, pl.ds(pl.multiple_of(p * W, W), W)]
                ).astype(BF16)
            remote(
                ysend.at[p, part], ybuf.at[tp, part], y_send, y_recv.at[half, tp], {"tp": p}
            ).start()
    act_n = act_d[0 : 2 * SN]
    part = dot(act_n, ed[...]).astype(BF16)
    wide = jnp.concatenate([stack(part[:, q * W : (q + 1) * W]) for q in range(NTP)], axis=1)
    turned = dot(permt_n[...], wide)
    for q in range(NTP):
        routn[:, q] = turned[:, 128 * q : 128 * q + 128].reshape(SN, 8, 128).astype(BF16)
    for b in range(NEAR):
        dz = ORDER[b]
        for i in range(1, NR + 1):
            if b or i < NR:
                m = mates[i % NR]
                remote(
                    routn.at[b * NR + m],
                    rinn.at[mine(b)],
                    c_send,
                    c_recv,
                    {"ep": planes[dz] * NR + m},
                ).start()
    rinn[r] = routn[r]

    own_cols = ed[:, pl.ds(pl.multiple_of(tp * W, W), W)]
    sum_b = dot(act_b, own_cols).astype(BF16).astype(F32)
    sum_a = dot(act_f, own_cols).astype(BF16).astype(F32)
    for half, lo, n, turn, first, last, rows in (
        (0, 0, SB, permt_b, 3, 5, sum_b),
        (2, 32, NR, permt_c, 7, 8, sum_a[32:48]),
        (1, 16, SB, permt_b, 5, 7, sum_a[0:32]),
    ):
        for p in peers:
            part = pl.ds(2 * lo, 2 * n)
            arrived(ybuf.at[p, part], y_recv.at[half, p])
            rows = rows + ybuf[p, part].astype(F32)
        turned = dot(turn[...], stack(rows.astype(BF16)))
        rout[pl.ds(lo, n)] = turned.reshape(n, 8, 128).astype(BF16)
        for b in reversed(range(first, last)):
            dz = ORDER[b]
            for i in range(1, NR + 1):
                m = mates[i % NR]
                remote(
                    rout.at[(b - NEAR) * NR + m],
                    rin.at[mine(b) - SN],
                    b_send,
                    b_recv.at[min(half, 1)],
                    {"ep": planes[dz] * NR + m},
                ).start()

    def routed(picked):
        return unstack(picked[0:64] * w_cols[0] + picked[64:128] * w_cols[1])

    arrived(rinn.at[pl.ds(0, SN - 1)], c_recv)
    wide = jnp.concatenate([rinn[:, q].reshape(8 * SN, 128) for q in range(NTP)], axis=1)
    picked = dot(rmat_n[...], wide)
    for q in range(NTP):
        part = routed(picked[:, 128 * q : 128 * q + 128])
        dpart[:, q * W : (q + 1) * W] = part + dpart[:, q * W : (q + 1) * W]
    for i in (2, 1, 3, 0):
        q = lax.rem(tp + i, NTP)
        part = dpart[:, pl.ds(pl.multiple_of(q * W, W), W)]
        if i:
            dsend[q] = part.astype(BF16)
            remote(dsend.at[q], dbuf.at[tp], d_send, d_recv.at[tp], {"tp": q}).start()
        else:
            mixed = residual.astype(F32) + part

    arrived(rin.at[pl.ds(0, SB)], b_recv.at[0])
    mixed = mixed + routed(dot(rmat_b[...], rin[pl.ds(0, SB)].reshape(8 * SB, 128)))
    for p in peers:
        arrived(dbuf.at[p], d_recv.at[p])
        mixed = mixed + dbuf[p].astype(F32)
    arrived(rin.at[pl.ds(SB, SA)], b_recv.at[1])
    mixed = mixed + routed(dot(rmat_f[...], rin[pl.ds(SB, SA)].reshape(8 * SA, 128)))
    out[...] = mixed.astype(BF16)

    left(xbuf.at[pl.ds(0, 3)], x_send)
    left(abuf.at[pl.ds(0, 3)], p_send)
    left(outg, o_send)
    left(outn.at[pl.ds(0, SD - 1)], n_send)
    left(gath.at[pl.ds(0, 3), pl.ds(SD, SA)], g_send)
    left(dsend.at[pl.ds(0, 3)], d_send)
    left(ysend.at[pl.ds(0, 3)], y_send)
    left(rout, b_send)
    left(routn.at[pl.ds(0, SN - 1)], c_send)


def local(
    tokens,
    kv_cache,
    cum_gate,
    lengths,
    w_query,
    w_key,
    w_value,
    w_forget,
    forget_bias,
    w_out,
    attn_gain,
    ffn_gain,
    mix_gate,
    expert_gate,
    expert_up,
    expert_down,
    chosen,
    route_weight,
    dense_gate,
    dense_up,
    dense_down,
):
    vmem = pl.BlockSpec(memory_space=pltpu.VMEM)
    hbm = pl.BlockSpec(memory_space=ANY)
    dma = pltpu.SemaphoreType.DMA
    regular = pltpu.SemaphoreType.REGULAR
    scratch = [
        pltpu.VMEM((TOK, W), BF16),
        pltpu.SMEM((TOK,), jnp.int32),
        pltpu.SMEM((4,), F32),
        pltpu.VMEM((16, 128), BF16),
        pltpu.VMEM((16, 128), BF16),
        pltpu.VMEM((16, 128), BF16),
        pltpu.VMEM((2, TOK), jnp.int32),
        pltpu.VMEM((2, TOK), F32),
        pltpu.VMEM((TOK, 1024, 128), BF16),
        pltpu.VMEM((4, 256, 1024), BF16),
        pltpu.VMEM((4, 1024, 256), BF16),
        pltpu.VMEM((TOK, 4, 1024), F32),
        pltpu.VMEM((2048, 256), BF16),
        pltpu.VMEM((128, 2048), BF16),
        pltpu.VMEM((4, 2048), BF16),
        pltpu.VMEM((256, 2048), BF16),
        pltpu.VMEM((2048, 256), BF16),
        pltpu.VMEM((2048, 256), BF16),
        pltpu.VMEM((256, 2048), BF16),
        pltpu.VMEM((2048, 256), BF16),
        pltpu.VMEM((2048, 256), BF16),
        pltpu.VMEM((256, 2048), BF16),
        pltpu.VMEM((NTP, TOK, W), BF16),
        pltpu.VMEM((64, 1024), F32),
        pltpu.VMEM((NTP, TOK, W), BF16),
        pltpu.VMEM((NTP, NTP, TOK, W), BF16),
        pltpu.VMEM((512, 64), BF16),
        pltpu.VMEM((128, 8 * SN), BF16),
        pltpu.VMEM((128, 8 * SB), BF16),
        pltpu.VMEM((128, 8 * SA), BF16),
        pltpu.VMEM((8 * SN, 8 * SN), BF16),
        pltpu.VMEM((8 * SN, 8 * SN), BF16),
        pltpu.VMEM((8 * SB, 8 * SB), BF16),
        pltpu.VMEM((8 * SB, 8 * SB), BF16),
        pltpu.VMEM((64, 64), BF16),
        pltpu.VMEM((NTP, TOK, W), BF16),
        pltpu.VMEM((SA, 8, 128), BF16),
        pltpu.VMEM((SD, NTP, 8, 128), BF16),
        pltpu.VMEM((NTP, NEP, 8, 128), BF16),
        pltpu.VMEM((128, 2048), BF16),
        pltpu.VMEM((TOK, 2048), F32),
        pltpu.VMEM((NTP, TOK, W), BF16),
        pltpu.VMEM((NTP, TOK, W), BF16),
        pltpu.VMEM((NTP, 2 * SF, W), BF16),
        pltpu.VMEM((NTP, 2 * SF, W), BF16),
        pltpu.VMEM((SF, 8, 128), BF16),
        pltpu.VMEM((SN, NTP, 8, 128), BF16),
        pltpu.VMEM((SF, 8, 128), BF16),
        pltpu.VMEM((SN, NTP, 8, 128), BF16),
        pltpu.VMEM((16, 128), F32),
        pltpu.VMEM((16, 128), F32),
        dma((20,)),
        dma((4,)),
        dma,
        dma((NTP,)),
        regular,
        regular,
        dma,
        dma((NTP,)),
        dma((NTP,)),
        dma,
        dma((NZ,)),
        dma,
        dma((NTP,)),
        dma,
        dma((NTP,)),
        dma,
        dma((3, NTP)),
        dma,
        dma((2,)),
        dma,
        dma,
        dma,
    ]
    return pl.pallas_call(
        layer,
        out_shape=pltpu.VMEM((TOK, W), BF16),
        in_specs=[hbm] * 21,
        out_specs=vmem,
        scratch_shapes=scratch,
        compiler_params=pltpu.CompilerParams(collective_id=0, has_side_effects=True),
        name="layer",
    )(
        tokens,
        lengths,
        forget_bias,
        attn_gain.reshape(16, 128),
        ffn_gain.reshape(16, 128),
        mix_gate.reshape(16, 128),
        chosen.T,
        route_weight.T,
        kv_cache,
        cum_gate,
        w_query,
        w_key.T,
        w_value.T,
        w_forget.T,
        w_out,
        expert_gate[0],
        expert_up[0],
        expert_down[0],
        dense_gate,
        dense_up,
        dense_down,
    )


def solution(mesh):
    in_specs = (
        P("ep", "tp"),
        P("ep", None, "tp"),
        P("ep", "tp", None),
        P("ep"),
        P(None, "tp"),
        P(None, "tp"),
        P(None, "tp"),
        P(None, "tp"),
        P("tp"),
        P("tp", None),
        P(),
        P(),
        P(),
        P("ep", None, "tp"),
        P("ep", None, "tp"),
        P("ep", "tp", None),
        P("ep", None),
        P("ep", None),
        P(None, "tp"),
        P(None, "tp"),
        P("tp", None),
    )
    out_specs = P("ep", "tp")
    return jax.shard_map(local, mesh=mesh, in_specs=in_specs, out_specs=out_specs, check_vma=False)
```
